256 devices in a mesh: sp: 32 (over z, y), fs: 4 (over x), tp: 2 (over core).
Axes of the slice: x: 4, y: 4, z: 8, core: 2. Of those that a mesh axis runs over, the one named last changes fastest.
Arguments:
- tokens: bfloat16 [4, 24576, 2048], P('fs', 'sp', 'tp'), may hold values from -6 to 6
- in_gain: float32 [2048], replicated, may hold values from 0.1 to 1.9
- ret_query: bfloat16 [2048, 768], P(None, 'tp'), may hold values from -0.125 to 0.125
- ret_key: bfloat16 [2048, 768], P(None, 'tp'), may hold values from -0.125 to 0.125
- ret_value: bfloat16 [2048, 768], P(None, 'tp'), may hold values from -0.125 to 0.125
- att_query: bfloat16 [2048, 768], P(None, 'tp'), may hold values from -8 to 8
- att_key: bfloat16 [2048, 256], P(None, 'tp'), may hold values from -8 to 8
- att_value: bfloat16 [2048, 256], P(None, 'tp'), may hold values from -0.125 to 0.125
- log_decay: float32 [4, 12, 24576], P('fs', 'tp', 'sp'), may hold values from -1.5 to 0
- ret_gain: float32 [768], P('tp'), may hold values from 0.1 to 1.9
- sink_logit: float32 [12], P('tp'), may hold values from 1 to 5
- retentive_exit_matrix: bfloat16 [768, 2048], P('tp'), may hold values from -0.15625 to 0.15625
- out_att: bfloat16 [768, 2048], P('tp'), may hold values from -0.875 to 0.875
Outputs:
- mixed: bfloat16 [4, 24576, 2048], P('fs', ('sp', 'tp'))
The draws below stay inside these ranges and needn't reach their ends.
All inputs are finite; a program needn't handle non-finite values.
Results may differ from the reference program's by a relative error of at most 0.0085.
Values may be sent and summed in bfloat16 or wider, within the bound.
A program may use at most 128 MiB of HBM per device.

```python
import jax
import jax.numpy as jnp
from jax import lax

D = 2048
HEAD_DIM = 64
RET_HEADS = 12
ATT_HEADS = 12
KV_HEADS = 4
WINDOW = 128
TOK_DEV = 768
SEQ = 24576
BATCH = 4


def paired_heads(key):
    keys = jax.random.split(jax.random.fold_in(key, 5), 2)
    key_weight = jax.random.normal(keys[0], (D, KV_HEADS * HEAD_DIM), jnp.float32) * D ** (-0.5)
    query_weight = jax.random.normal(keys[1], (D, ATT_HEADS * HEAD_DIM), jnp.float32) * D ** (-0.5)
    return (jnp.clip(query_weight, -8.0, 8.0), jnp.clip(key_weight, -8.0, 8.0))


def draw_att_query(key, part):
    return paired_heads(key)[0].astype(jnp.bfloat16)


def draw_att_key(key, part):
    return paired_heads(key)[1].astype(jnp.bfloat16)


def draw_log_decay(key, part):
    keys = jax.random.split(jax.random.fold_in(key, 11), 5)
    keep_share = 0.5
    slow = jax.random.uniform(keys[0], (BATCH, RET_HEADS, 1), jnp.float32) < keep_share
    span = 30.0 * jnp.exp(jax.random.uniform(keys[1], (BATCH, RET_HEADS, 1), jnp.float32) * jnp.log(100.0 / 30.0))
    starting_shift_amount = jnp.where(slow, -jnp.log(10.0) / (4.0 * SEQ), -1.0 / span)
    blocks = SEQ // TOK_DEV
    fading_multiplier = jnp.exp(jax.random.uniform(keys[2], (BATCH, 1, blocks), jnp.float32) * jnp.log(3.0))
    fading_multiplier = jnp.repeat(fading_multiplier, TOK_DEV, axis=2)
    location_numbers = jax.random.randint(keys[3], (BATCH, 3, 1), 0, SEQ)
    objective_numbers = jnp.log(1.0 - jax.random.uniform(keys[4], (BATCH, 3, 1), jnp.float32, 0.2, 0.5))
    element_locations = jnp.arange(SEQ)[None, None, :]
    cluster_sets = jnp.sum(jnp.where(element_locations == location_numbers, objective_numbers, 0.0), axis=1, keepdims=True)
    return (starting_shift_amount * fading_multiplier + cluster_sets).astype(jnp.float32)


def block_scale(key, dims, cuts, least, largest):
    def one(axis_at, shards_of):
        heights = jax.random.uniform(jax.random.fold_in(jax.random.fold_in(key, 6), axis_at), (shards_of,), jnp.float32, least / len(cuts), largest / len(cuts))
        return jnp.repeat(jnp.exp(heights), dims[axis_at] // shards_of).reshape((-1,) + (1,) * (len(dims) - axis_at - 1))

    level = one(*cuts[0])
    for cut in cuts[1:]:
        level = level * one(*cut)
    return level


def gaussian(key, dims, width, reach, pieces=(), held_as=jnp.bfloat16):
    array = jax.random.normal(key, dims, jnp.float32) * width
    if len(pieces) > 0:
        array = block_scale(key, dims, pieces, -0.22, 0.18) * array
    return jnp.clip(array, min=-reach, max=reach).astype(held_as)


def setup_inputs(seed: int = 0) -> dict:
    arg_keys = jax.random.split(jax.random.key(seed), 14)
    tokens = gaussian(arg_keys[0], (BATCH, SEQ, D), 1.0, 6.0, ((0, 4), (1, 32), (2, 2)))
    in_gain = jnp.clip(1.0 + 0.18 * jax.random.normal(arg_keys[1], (D,), jnp.float32), 0.1, 1.9)
    ret_query = gaussian(arg_keys[2], (D, RET_HEADS * HEAD_DIM), D ** -0.5, 0.125, ((1, 2),))
    ret_key = gaussian(arg_keys[3], (D, RET_HEADS * HEAD_DIM), D ** -0.5, 0.125, ((1, 2),))
    ret_value = gaussian(arg_keys[4], (D, RET_HEADS * HEAD_DIM), D ** -0.5, 0.125, ((1, 2),))
    att_query = draw_att_query(jax.random.fold_in(arg_keys[13], 71), 0)
    att_key = draw_att_key(jax.random.fold_in(arg_keys[13], 71), 0)
    att_value = gaussian(arg_keys[7], (D, KV_HEADS * HEAD_DIM), D ** -0.5, 0.125, ((1, 2),))
    log_decay = draw_log_decay(jax.random.fold_in(arg_keys[13], 71), 0)
    ret_gain = jnp.clip(1.0 + 0.18 * jax.random.normal(arg_keys[9], (RET_HEADS * HEAD_DIM,), jnp.float32), 0.1, 1.9)
    sink_logit = jnp.clip(1.0 + 4.0 * jax.random.uniform(arg_keys[10], (ATT_HEADS,), jnp.float32) ** block_scale(arg_keys[10], (ATT_HEADS,), ((0, 2),), -0.2, 0.2), 1.0, 5.0)
    retentive_exit_matrix = gaussian(arg_keys[11], (RET_HEADS * HEAD_DIM, D), (2 * RET_HEADS * HEAD_DIM) ** -0.5, 0.15625, ((0, 2),))
    out_att = gaussian(arg_keys[12], (ATT_HEADS * HEAD_DIM, D), (ATT_HEADS * HEAD_DIM // 16) ** -0.5, 0.875, ((0, 2),))
    return dict(tokens=tokens, in_gain=in_gain, ret_query=ret_query, ret_key=ret_key, ret_value=ret_value, att_query=att_query, att_key=att_key, att_value=att_value, log_decay=log_decay, ret_gain=ret_gain, sink_logit=sink_logit, retentive_exit_matrix=retentive_exit_matrix, out_att=out_att)


EPS = 1e-06

def retention_sequence(query_rows, key_rows, value_rows, log_rates, gain):
    heads = log_rates.shape[0]
    blocks = query_rows.shape[0] // TOK_DEV
    fading_multiplier = HEAD_DIM ** (-0.5)
    shaped_q = query_rows.reshape(blocks, TOK_DEV, heads, HEAD_DIM)
    shaped_k = key_rows.reshape(blocks, TOK_DEV, heads, HEAD_DIM)
    shaped_v = value_rows.reshape(blocks, TOK_DEV, heads, HEAD_DIM)
    shaped_r = log_rates.reshape(heads, blocks, TOK_DEV).transpose(1, 0, 2)
    later = jnp.arange(TOK_DEV)[:, None] >= jnp.arange(TOK_DEV)[None, :]

    def advance(state, inputs):
        block_q, block_k, block_v, block_r = inputs
        cumulative = jnp.cumsum(block_r, axis=1)
        decay = jnp.exp(jnp.where(later[None], cumulative[:, :, None] - cumulative[:, None, :], -jnp.inf))
        query_f = block_q.astype(jnp.float32)
        key_f = block_k.astype(jnp.float32)
        value_f = block_v.astype(jnp.float32)
        weights = (jnp.einsum('thd,shd->hts', query_f, key_f) * fading_multiplier * decay).astype(jnp.bfloat16)
        inner = jnp.einsum('hts,shd->thd', weights.astype(jnp.float32), value_f)
        carried = jnp.einsum('thd,hde->the', query_f, state, precision=lax.Precision.HIGHEST)
        carried = carried * jnp.exp(cumulative).T[:, :, None]
        keyed = key_f * (jnp.exp(cumulative[:, -1:] - cumulative) * fading_multiplier).T[:, :, None]
        own_state = jnp.einsum('shd,she->hde', keyed, value_f, precision=lax.Precision.HIGHEST)
        state = jnp.exp(cumulative[:, -1])[:, None, None] * state + own_state
        return (state, inner + carried)
    start_state = jnp.zeros((heads, HEAD_DIM, HEAD_DIM), jnp.float32)
    _, outputs = lax.scan(advance, start_state, (shaped_q, shaped_k, shaped_v, shaped_r))
    outputs = outputs.reshape(-1, heads, HEAD_DIM)
    normed = outputs * lax.rsqrt(lax.optimization_barrier(jnp.mean(outputs * outputs, axis=-1, keepdims=True)) + EPS)
    return (normed.reshape(-1, heads * HEAD_DIM) * gain).astype(jnp.bfloat16)

def window_attention(query_rows, key_ext, value_ext, first_position, sinks):
    length = query_rows.shape[0]
    blocks = length // WINDOW
    heads_kv = key_ext.shape[1] // HEAD_DIM
    heads = query_rows.shape[1] // HEAD_DIM
    group = heads // heads_kv
    shaped_q = query_rows.astype(jnp.float32).reshape(blocks, WINDOW, heads_kv, group, HEAD_DIM)
    key_block_list = key_ext.astype(jnp.float32).reshape(blocks + 1, WINDOW, heads_kv, HEAD_DIM)
    value_blocks = value_ext.astype(jnp.float32).reshape(blocks + 1, WINDOW, heads_kv, HEAD_DIM)
    key_band = jnp.concatenate([key_block_list[:-1], key_block_list[1:]], axis=1)
    value_band = jnp.concatenate([value_blocks[:-1], value_blocks[1:]], axis=1)
    scores = jnp.einsum('nqhgd,nkhd->hgnqk', shaped_q, key_band) * HEAD_DIM ** (-0.5)
    distance = WINDOW + jnp.arange(WINDOW)[:, None] - jnp.arange(2 * WINDOW)[None, :]
    key_position = first_position - WINDOW + jnp.arange(blocks)[:, None] * WINDOW + jnp.arange(2 * WINDOW)[None, :]
    allowed = ((distance >= 0) & (distance < WINDOW))[None] & (key_position >= 0)[:, None, :]
    scores = jnp.where(allowed, scores, -jnp.inf)
    sink_part = sinks.reshape(heads_kv, group, 1, 1, 1)
    greatest_level = jnp.maximum(lax.optimization_barrier(jnp.max(scores, axis=-1, keepdims=True)), sink_part)
    raised = jnp.exp(scores - greatest_level)
    totals = lax.optimization_barrier(jnp.sum(raised, axis=-1, keepdims=True)) + jnp.exp(sink_part - greatest_level)
    weights = (raised / totals).astype(jnp.bfloat16)
    outputs = jnp.einsum('hgnqk,nkhd->nqhgd', weights.astype(jnp.float32), value_band)
    return outputs.reshape(length, heads * HEAD_DIM).astype(jnp.bfloat16)

def reference(tokens, in_gain, ret_query, ret_key, ret_value, att_query, att_key, att_value, log_decay, ret_gain, sink_logit, retentive_exit_matrix, out_att):
    results = []
    for sequence in range(tokens.shape[0]):
        wide = tokens[sequence].astype(jnp.float32)
        inverse = lax.rsqrt(lax.optimization_barrier(jnp.mean(wide * wide, axis=-1, keepdims=True)) + EPS)
        scaled = (wide * in_gain).astype(jnp.bfloat16)

        def project(weight):
            return (jnp.dot(scaled, weight, preferred_element_type=jnp.float32) * inverse).astype(jnp.bfloat16)
        ret_q = project(ret_query)
        ret_k = project(ret_key)
        ret_v = project(ret_value)
        att_q = project(att_query)
        att_k = project(att_key)
        att_v = project(att_value)
        ret_out = retention_sequence(ret_q, ret_k, ret_v, log_decay[sequence], ret_gain)
        padding = jnp.zeros((WINDOW, att_k.shape[1]), jnp.bfloat16)
        att_out = window_attention(att_q, jnp.concatenate([padding, att_k], axis=0), jnp.concatenate([padding, att_v], axis=0), 0, sink_logit)
        summed = jnp.dot(ret_out, retentive_exit_matrix, preferred_element_type=jnp.float32) + jnp.dot(att_out, out_att, preferred_element_type=jnp.float32)
        results.append(summed.astype(jnp.bfloat16))
    return jnp.stack(results)
```

```python
import functools

import jax
import jax.numpy as jnp
from jax import lax
from jax.experimental import pallas as pl
from jax.experimental.pallas import tpu as pltpu
from jax.sharding import PartitionSpec as P

EPS = 1e-06
D = 2048
T = 768
HALF = 384
C = 128
NC = 6
NEG = float("-inf")
f32 = jnp.float32
bf16 = jnp.bfloat16


def dot(a, b):
    return jnp.dot(a, b, preferred_element_type=f32)


def dot_t(a, b):
    return lax.dot_general(a, b, (((1,), (1,)), ((), ())), preferred_element_type=f32)


def t_dot(a, b):
    return lax.dot_general(a, b, (((0,), (0,)), ((), ())), preferred_element_type=f32)


def split3(x):
    a = x.astype(bf16).astype(f32)
    r = x - a
    b = r.astype(bf16).astype(f32)
    return a, b, (r - b).astype(bf16).astype(f32)


def iota(shape, dim):
    return lax.broadcasted_iota(jnp.int32, shape, dim)


def kernel(
    tok, gain, wrq, wrk, wrv, waq, wak, wav, ld, rgain, sink, wre, wao,
    out,
    gain_v, rgain_v, sink_v, ld_v,
    tok_o, tok_p, sc_o, ssq,
    wkv, wq, wa, acc_kv, acc_q, acc_a,
    kv, qb, akv, qs,
    lcrow, lch, el, tots, et, st, inner,
    wmask, biasc,
    st_a, buf_a, l_a, buf_al, g_b, buf_b, l_b, buf_bl, s_c, buf_c,
    wo, att, att_p, ret, ret_p, oacc,
    lsem, tsem, trec, wsem, wrec, hsem, hrec,
    asem, arec, alsem, alrec, bsem, brec, blsem, blrec, csem, crec, osem, orec,
):
    sp = lax.axis_index("sp")
    tp = lax.axis_index("tp")
    y = lax.rem(sp, 4)
    z = lax.div(sp, 4)
    other = 1 - tp
    peer = {"tp": other}
    y_at = [lax.rem(y + d, 4) for d in range(4)]
    z_at = [lax.rem(z + d, 8) for d in range(8)]

    def at_y(d):
        return {"sp": z * 4 + y_at[d]}

    def at_z(d):
        return {"sp": z_at[d] * 4 + y}

    nxt = {"sp": lax.rem(sp + 1, 32)}
    prv = {"sp": lax.rem(sp + 31, 32)}

    barrier = pltpu.get_barrier_semaphore()
    greet = [peer] + [at_y(d) for d in range(1, 4)] + [at_z(d) for d in range(1, 8)] + [prv]
    for who in greet:
        pl.semaphore_signal(barrier, inc=1, device_id=who, device_id_type=pl.DeviceIdType.MESH)

    local = []

    def load(src, dst):
        cp = pltpu.make_async_copy(src, dst, lsem.at[len(local)])
        cp.start()
        local.append(cp)
        return cp

    own = pl.ds(pl.multiple_of(tp * 1024, 1024), 1024)
    oth = pl.ds(pl.multiple_of(other * 1024, 1024), 1024)
    here, there = pl.ds(0, 1024), pl.ds(1024, 1024)

    def load2(a, b, rows, dst, to, w):
        return [load(a.at[rows], dst.at[to, pl.ds(0, w)]), load(b.at[rows], dst.at[to, pl.ds(w, w)])]

    c_tok = load(tok.at[0], tok_o)
    c_ld = [load(ld.at[h], ld_v.at[pl.ds(h, 1)]) for h in range(6)]
    c_gain = load(gain, gain_v)
    c_kv = load2(wrk, wrv, own, wkv, here, 384)

    lane1 = iota((1, 128), 1)
    m0 = jnp.where(lane1 < 64, 1.0, 0.0).astype(bf16)
    m1 = jnp.where(lane1 < 64, 0.0, 1.0).astype(bf16)
    wmask[0:C] = jnp.where(iota((C, C), 0) > iota((C, C), 1), 1.0, 0.0).astype(bf16)
    wmask[C:] = jnp.where(iota((C, C), 0) > iota((C, C), 1), 0.0, 1.0).astype(bf16)
    biasc[...] = jnp.where(iota((C, C), 0) >= iota((C, C), 1), 0.0, NEG)

    for cp in c_ld:
        cp.wait()
    raw = ld_v[...]
    rows48 = jnp.concatenate([raw[:, c * C:(c + 1) * C] for c in range(NC)], axis=0)
    rows48 = jnp.where(lax.rem(iota((48, C), 0), 8) < 6, rows48, 0.0)
    upper = jnp.where(iota((C, C), 0) <= iota((C, C), 1), 1.0, 0.0).astype(bf16)
    parts = jnp.concatenate(split3(rows48), axis=0).astype(bf16)
    summed = dot(parts, upper)
    lc = summed[0:48] + summed[48:96] + summed[96:144]
    lcrow[...] = lc
    sr, sl = lax.rem(iota((24, 1152), 0), 8), iota((24, 1152), 1)
    head_of = jnp.where(sl < 384, lax.div(sl, 64), lax.div(sl - 384, 128))
    sel = jnp.where(sr == head_of, 1.0, 0.0).astype(bf16)
    before = jnp.zeros((1, 384), f32)
    for c in range(NC):
        p3 = jnp.concatenate(split3(lc[c * 8:(c + 1) * 8]), axis=0).astype(bf16)
        cols = t_dot(p3, sel)
        lch[pl.ds(c * C, C)] = cols[:, 384:]
        el[pl.ds(c * C, C)] = cols[:, :384]
        last = cols[C - 1:C, :384]
        tots[c:c + 1] = last
        et[c:c + 1] = jnp.exp(before)
        before = before + last
    for p in range(3):
        l_a[p:p + 1] = before[:, p * 128:(p + 1) * 128]

    c_gain.wait()
    c_tok.wait()
    c_a = load2(wak, wav, own, wa, here, 128)
    c_q = load2(wrq, waq, own, wq, here, 384)
    g_o = gain_v[:, own]
    g_p = gain_v[:, oth]

    def scale_rows(src, r0, g):
        x = src[pl.ds(r0, 64)].astype(f32)
        sq = x * x
        part = sq[:, 0:128]
        for j in range(1, 8):
            part = part + sq[:, j * 128:(j + 1) * 128]
        return (x * g).astype(bf16), part

    def own_rows(i, carry):
        r0 = pl.multiple_of(i * 64, 64)
        s, part = scale_rows(tok_o, r0, g_o)
        sc_o[pl.ds(r0, 64)] = s
        ssq[pl.ds(r0, 64)] = part
        return carry

    lax.fori_loop(0, T // 64, own_rows, 0)

    pl.semaphore_wait(barrier, len(greet))

    t_cp = []
    for r in range(2):
        rows = pl.ds(r * HALF, HALF)
        cp = pltpu.make_async_remote_copy(
            src_ref=tok.at[0, rows], dst_ref=tok_p.at[rows], send_sem=tsem.at[r], recv_sem=trec.at[r],
            device_id=peer, device_id_type=pl.DeviceIdType.MESH)
        cp.start()
        t_cp.append(cp)
    w_cp = []
    for i, w in enumerate((wre, wao)):
        cp = pltpu.make_async_remote_copy(
            src_ref=w, dst_ref=wo.at[i, pl.ds(384, 384)], send_sem=wsem.at[i], recv_sem=wrec.at[i],
            device_id=peer, device_id_type=pl.DeviceIdType.MESH)
        cp.start()
        w_cp.append(cp)

    c_kv2 = load2(wrk, wrv, oth, wkv, there, 384)
    c_a2 = load2(wak, wav, oth, wa, there, 128)
    c_q2 = load2(wrq, waq, oth, wq, there, 384)
    c_small = [load(rgain, rgain_v), load(sink, sink_v)]
    c_wo = [load(wre, wo.at[0, pl.ds(0, 384)]), load(wao, wo.at[1, pl.ds(0, 384)])]

    def first_half(acc, w):
        for r in range(2):
            rows = pl.ds(r * HALF, HALF)
            acc[rows] = dot(sc_o[rows], w[here])

    def wait_all(cps):
        for cp in cps:
            cp.wait()

    wait_all(c_kv)
    first_half(acc_kv, wkv)
    wait_all(c_a)
    first_half(acc_a, wa)
    wait_all(c_q)
    first_half(acc_q, wq)

    inv = [None, None]
    wait_all(c_kv2)
    for r in range(2):
        t_cp[r].wait_recv()

        def peer_rows(i, carry):
            r0 = pl.multiple_of(r * HALF + i * 64, 64)
            s, part = scale_rows(tok_p, r0, g_p)
            tok_p[pl.ds(r0, 64)] = s
            total = jnp.sum(ssq[pl.ds(r0, 64)] + part, axis=1, keepdims=True)
            ssq[pl.ds(r0, 64)] = jnp.broadcast_to(lax.rsqrt(total / D + EPS), (64, 128))
            return carry

        lax.fori_loop(0, HALF // 64, peer_rows, 0)
        rows = pl.ds(r * HALF, HALF)
        res = acc_kv[rows] + dot(tok_p[rows], wkv[there])
        kv[rows] = (res * ssq[rows, 0:1]).astype(bf16)

    lo = iota((64, 128), 1) < 64
    s_p = [jnp.zeros((64, 128), f32) for _ in range(3)]
    for c in range(NC):
        rows = pl.ds(c * C, C)
        tot = tots[c:c + 1]
        for p in range(3):
            cols = pl.ds(p * 128, 128)
            tp_ = tot[:, p * 128:(p + 1) * 128]
            lcp = el[rows, cols]
            kd = (kv[rows, cols].astype(f32) * jnp.exp(tp_ - lcp)).astype(bf16)
            m = t_dot(kd, kv[rows, pl.ds(384 + p * 128, 128)])
            comp = jnp.where(lo, m[0:64], m[64:128])
            st[c, p] = s_p[p].astype(bf16)
            s_p[p] = jnp.exp(tp_) * s_p[p] + comp
    for p in range(3):
        for q in range(4):
            st_a[q, p] = s_p[p][q * 16:(q + 1) * 16].astype(bf16)

    a_cp, al_cp = [], []

    def send(src, dst, ss, rs, who, group):
        cp = pltpu.make_async_remote_copy(
            src_ref=src, dst_ref=dst, send_sem=ss, recv_sem=rs, device_id=who,
            device_id_type=pl.DeviceIdType.MESH)
        cp.start()
        group.append(cp)

    def arrived(src, dst, ss, rs, who):
        pltpu.make_async_remote_copy(
            src_ref=src, dst_ref=dst, send_sem=ss, recv_sem=rs, device_id=who,
            device_id_type=pl.DeviceIdType.MESH).wait_recv()

    for d in range(1, 4):
        send(st_a.at[y_at[d]], buf_a.at[y], asem.at[d - 1], arec.at[y], at_y(d), a_cp)
        send(l_a, buf_al.at[y], alsem.at[d - 1], alrec.at[y], at_y(d), al_cp)
    buf_a[y] = st_a[y]
    buf_al[y] = l_a[...]

    wait_all(c_a2)
    for r in range(2):
        rows = pl.ds(r * HALF, HALF)
        res = acc_a[rows] + dot(tok_p[rows], wa[there])
        akv[pl.ds(C + r * HALF, HALF)] = (res * ssq[rows, 0:1]).astype(bf16)
    halo = pltpu.make_async_remote_copy(
        src_ref=akv.at[pl.ds(T, C)], dst_ref=akv.at[pl.ds(0, C)], send_sem=hsem, recv_sem=hrec,
        device_id=nxt, device_id_type=pl.DeviceIdType.MESH)
    halo.start()
    wait_all(c_q2)
    for r in range(2):
        rows = pl.ds(r * HALF, HALF)
        res = acc_q[rows] + dot(tok_p[rows], wq[there])
        res = res * (ssq[rows, 0:1] * 0.125)
        qb[rows] = res[:, :384].astype(bf16)
        for p in range(3):
            two = res[:, 384 + p * 128:384 + (p + 1) * 128]
            swapped = pltpu.roll(two, 64, 1) if p != 1 else two
            for j in range(2):
                h = 2 * p + j
                val = ((swapped if h in (1, 4) else two).astype(bf16)) * (m0 if h < 3 else m1)
                for b in range(3):
                    qs[r * 3 + b, pl.ds(h * C, C)] = val[b * C:(b + 1) * C]

    def spread(s):
        return jnp.concatenate([s * m0, s * m1], axis=0)

    def ret_chunk(c, carry):
        rows = pl.ds(pl.multiple_of(c * C, C), C)
        past = et[pl.ds(c, 1)]
        lrows = lcrow[pl.ds(pl.multiple_of(c * 8, 8), 8)]
        for p in range(3):
            cols = pl.ds(p * 128, 128)
            q2, k2, v2 = qb[rows, cols], kv[rows, cols], kv[rows, pl.ds(384 + p * 128, 128)]
            ws = []
            for j, mj in enumerate((m0, m1)):
                h = 2 * p + j
                gap = lch[rows, pl.ds(h * 128, 128)] - lrows[h:h + 1] + biasc[...]
                ws.append((dot_t(q2 * mj, k2) * jnp.exp(gap)).astype(bf16))
            ex = jnp.exp(el[rows, cols])
            el[rows, cols] = ex * past[:, p * 128:(p + 1) * 128]
            ws.append((q2.astype(f32) * ex).astype(bf16))
            rhs = jnp.concatenate([v2 * m0, v2 * m1, spread(st[c, p])], axis=0)
            inner[rows, cols] = dot(jnp.concatenate(ws, axis=1), rhs)
        return carry

    lax.fori_loop(0, NC, ret_chunk, 0)

    for d in range(1, 4):
        arrived(st_a.at[0], buf_a.at[y_at[d]], asem.at[d - 1], arec.at[y_at[d]], at_y(d))
        arrived(l_a, buf_al.at[y_at[d]], alsem.at[d - 1], alrec.at[y_at[d]], at_y(d))
    b_cp, bl_cp = [], []
    for p in range(3):
        e = jnp.zeros((16, 128), f32)
        ltot = jnp.zeros((1, 128), f32)
        for yy in range(4):
            lyy = buf_al[yy][p:p + 1]
            e = jnp.exp(lyy) * e + buf_a[yy, p].astype(f32)
            ltot = ltot + lyy
        g_b[p] = e.astype(bf16)
        l_b[p:p + 1] = ltot
    for d in range(1, 8):
        send(g_b, buf_b.at[z], bsem.at[d - 1], brec.at[z], at_z(d), b_cp)
        send(l_b, buf_bl.at[z], blsem.at[d - 1], blrec.at[z], at_z(d), bl_cp)
    buf_b[z] = g_b[...]
    buf_bl[z] = l_b[...]

    wait_all(c_small)
    halo.wait_recv()
    sink_row = jnp.concatenate(
        [jnp.broadcast_to(sink_v[0:1, h:h + 1], (1, C)) for h in range(6)], axis=1)

    def att_block(i, half):
        n = half * 3 + i
        bandr = pl.ds(pl.multiple_of(n * C, C), 2 * C)
        edge = (n == 0) & (sp == 0)
        s = dot_t(akv[bandr, pl.ds(0, 128)], qs[n])
        is_own = iota((C, C), 0) <= iota((C, C), 1)
        ws, scale = [], []
        for h in range(6):
            hc = slice(h * C, (h + 1) * C)
            past = jnp.where(edge, NEG, s[:C, hc])
            v = jnp.where(is_own, s[C:, hc], past)
            sk = sink_row[:, hc]
            top = jnp.maximum(jnp.max(v, axis=0, keepdims=True), sk)
            e = jnp.exp(v - top)
            scale.append(1.0 / (jnp.sum(e, axis=0, keepdims=True) + jnp.exp(sk - top)))
            eb = e.astype(bf16)
            ws.append(jnp.concatenate([eb * wmask[0:C], eb * wmask[C:]], axis=0))
        o = t_dot(akv[bandr, pl.ds(128, 128)], jnp.concatenate(ws, axis=1))
        cols = pl.ds(pl.multiple_of(i * C, C), C)
        for h in range(6):
            r0 = 64 if h >= 3 else 0
            att[half, pl.ds(h * 64, 64), cols] = (
                o[r0:r0 + 64, h * C:(h + 1) * C] * scale[h]).astype(bf16)
        return half

    mine = pl.ds(pl.multiple_of(tp * HALF, HALF), HALF)
    theirs = pl.ds(pl.multiple_of(other * HALF, HALF), HALF)
    o_cp = []
    lax.fori_loop(0, 3, att_block, other)
    send(att.at[other], att_p, osem.at[0], orec.at[0], peer, o_cp)
    lax.fori_loop(0, 3, att_block, tp)

    for d in range(1, 8):
        arrived(g_b, buf_b.at[z_at[d]], bsem.at[d - 1], brec.at[z_at[d]], at_z(d))
        arrived(l_b, buf_bl.at[z_at[d]], blsem.at[d - 1], blrec.at[z_at[d]], at_z(d))
    for p in range(3):
        e = jnp.zeros((16, 128), f32)
        for zz in range(7):
            step = jnp.exp(buf_bl[zz][p:p + 1]) * e + buf_b[zz, p].astype(f32)
            e = jnp.where(zz < z, step, e)
        for yy in range(4):
            s_c[yy, p] = e.astype(bf16)
            e = jnp.exp(buf_al[yy][p:p + 1]) * e + buf_a[yy, p].astype(f32)
    c_cp = []
    for d in range(1, 4):
        send(s_c.at[y_at[d]], buf_c.at[y], csem.at[d - 1], crec.at[y], at_y(d), c_cp)
    buf_c[y] = s_c[y]

    wait_all(c_wo)
    w_cp[0].wait_recv()
    w_cp[1].wait_recv()
    o_cp[0].wait_recv()
    lhs = jnp.concatenate([att[tp], att_p[...]], axis=0)
    for j in range(4):
        cols = pl.ds(j * 512, 512)
        oacc[:, cols] = t_dot(lhs, wo[1, :, cols])

    for d in range(1, 4):
        arrived(s_c.at[0], buf_c.at[y_at[d]], csem.at[d - 1], crec.at[y_at[d]], at_y(d))
    big = [spread(jnp.concatenate([buf_c[q, p] for q in range(4)], axis=0)) for p in range(3)]
    ones_bd = jnp.where(
        lax.div(iota((128, 128), 0), 64) == lax.div(iota((128, 128), 1), 64), 1.0, 0.0).astype(bf16)

    def finish(rows):
        for p in range(3):
            cols = pl.ds(p * 128, 128)
            full = inner[rows, cols] + dot(qb[rows, cols], big[p]) * el[rows, cols]
            ms = dot((full * full).astype(bf16), ones_bd) * (1.0 / 64)
            ret[rows, cols] = (full * lax.rsqrt(ms + EPS) * rgain_v[cols].reshape(1, 128)).astype(bf16)

    finish(theirs)
    send(ret.at[theirs], ret_p, osem.at[1], orec.at[1], peer, o_cp)
    finish(mine)
    o_cp[1].wait_recv()
    lhs = jnp.concatenate([ret[mine], ret_p[...]], axis=1)
    for j in range(4):
        cols = pl.ds(j * 512, 512)
        out[0, :, cols] = (oacc[:, cols] + dot(lhs, wo[0, :, cols])).astype(bf16)

    for cp in t_cp + w_cp + a_cp + al_cp + b_cp + bl_cp + c_cp + o_cp + [halo]:
        cp.wait_send()


def shards(tokens, in_gain, ret_query, ret_key, ret_value, att_query, att_key, att_value,
           log_decay, ret_gain, sink_logit, retentive_exit_matrix, out_att):
    hbm = pl.BlockSpec(memory_space=pltpu.HBM)
    V = pltpu.VMEM
    DMA = pltpu.SemaphoreType.DMA
    scratch = [
        V((1, D), f32), V((384,), f32), V((1, 6), f32), V((8, T), f32),
        V((T, 1024), bf16), V((T, 1024), bf16), V((T, 1024), bf16), V((T, 128), f32),
        V((D, 768), bf16), V((D, 768), bf16), V((D, 256), bf16),
        V((T, 768), f32), V((T, 768), f32), V((T, 256), f32),
        V((T, 768), bf16), V((T, 384), bf16), V((T + C, 256), bf16), V((NC, 768, 128), bf16),
        V((48, 128), f32), V((T, 768), f32), V((T, 384), f32), V((8, 384), f32), V((8, 384), f32),
        V((NC, 3, 64, 128), bf16), V((T, 384), f32),
        V((2 * C, C), bf16), V((C, C), f32),
        V((4, 3, 16, 128), bf16), V((4, 3, 16, 128), bf16), V((8, 128), f32), V((4, 8, 128), f32),
        V((3, 16, 128), bf16), V((8, 3, 16, 128), bf16), V((8, 128), f32), V((8, 8, 128), f32),
        V((4, 3, 16, 128), bf16), V((4, 3, 16, 128), bf16),
        V((2, 768, D), bf16), V((2, 384, HALF), bf16), V((384, HALF), bf16), V((T, 384), bf16),
        V((HALF, 384), bf16), V((HALF, D), f32),
        DMA((24,)), DMA((2,)), DMA((2,)), DMA((2,)), DMA((2,)), DMA(()), DMA(()),
        DMA((3,)), DMA((4,)), DMA((3,)), DMA((4,)), DMA((7,)), DMA((8,)), DMA((7,)), DMA((8,)),
        DMA((3,)), DMA((4,)), DMA((2,)), DMA((2,)),
    ]
    return pl.pallas_call(
        kernel,
        out_shape=jax.ShapeDtypeStruct((1, HALF, D), bf16),
        in_specs=[hbm] * 13,
        out_specs=pl.BlockSpec(memory_space=pltpu.VMEM),
        scratch_shapes=scratch,
        compiler_params=pltpu.CompilerParams(
            collective_id=0, has_side_effects=True, vmem_limit_bytes=48 * 1024 * 1024),
    )(*(pltpu.with_memory_space_constraint(arg, pltpu.HBM) for arg in (
        tokens, in_gain.reshape(1, D), ret_query, ret_key, ret_value, att_query, att_key, att_value,
        jnp.transpose(log_decay, (1, 0, 2)), ret_gain, sink_logit.reshape(1, 6), retentive_exit_matrix, out_att,
    )))


def solution(mesh):
    placed = (
        P("fs", "sp", "tp"), P(), P(None, "tp"), P(None, "tp"), P(None, "tp"), P(None, "tp"),
        P(None, "tp"), P(None, "tp"), P("fs", "tp", "sp"), P("tp"), P("tp"), P("tp", None), P("tp", None),
    )
    return jax.shard_map(
        shards, mesh=mesh, in_specs=placed, out_specs=P("fs", ("sp", "tp"), None), check_vma=False)
```

```python
import functools

import jax
import jax.numpy as jnp
from jax import lax
from jax.experimental import pallas as pl
from jax.experimental.pallas import tpu as pltpu
from jax.sharding import PartitionSpec as P

EPS = 1e-06
D = 2048
T = 768
HALF = 384
C = 128
NC = 6
NEG = float("-inf")
f32 = jnp.float32
bf16 = jnp.bfloat16


def dot(a, b):
    return jnp.dot(a, b, preferred_element_type=f32)


def dot_t(a, b):
    return lax.dot_general(a, b, (((1,), (1,)), ((), ())), preferred_element_type=f32)


def t_dot(a, b):
    return lax.dot_general(a, b, (((0,), (0,)), ((), ())), preferred_element_type=f32)


def split3(x):
    a = x.astype(bf16).astype(f32)
    r = x - a
    b = r.astype(bf16).astype(f32)
    return a, b, (r - b).astype(bf16).astype(f32)


def iota(shape, dim):
    return lax.broadcasted_iota(jnp.int32, shape, dim)


def kernel(
    tok, gain, wrq, wrk, wrv, waq, wak, wav, ld, rgain, sink, wre, wao,
    out,
    gain_v, rgain_v, sink_v, ld_v,
    tok_o, tok_p, sc_o, ssq,
    wkv, wq, wa, acc_kv, acc_a,
    kv, qb, akv, qs,
    lcrow, lch, el, tots, et, st, inner,
    wmask, biasc,
    st_a, buf_a, l_a, buf_al, g_b, buf_b, l_b, buf_bl, s_c, buf_c,
    wo, att, att_p, ret, ret_p, oacc,
    lsem, tsem, trec, wsem, wrec, hsem, hrec,
    asem, arec, alsem, alrec, bsem, brec, blsem, blrec, csem, crec, osem, orec,
):
    sp = lax.axis_index("sp")
    tp = lax.axis_index("tp")
    y = lax.rem(sp, 4)
    z = lax.div(sp, 4)
    other = 1 - tp
    peer = {"tp": other}
    y_at = [lax.rem(y + d, 4) for d in range(4)]
    z_at = [lax.rem(z + d, 8) for d in range(8)]

    def at_y(d):
        return {"sp": z * 4 + y_at[d]}

    def at_z(d):
        return {"sp": z_at[d] * 4 + y}

    nxt = {"sp": lax.rem(sp + 1, 32)}
    prv = {"sp": lax.rem(sp + 31, 32)}

    barrier = pltpu.get_barrier_semaphore()
    greet = [peer] + [at_y(d) for d in range(1, 4)] + [at_z(d) for d in range(1, 8)] + [prv]
    for who in greet:
        pl.semaphore_signal(barrier, inc=1, device_id=who, device_id_type=pl.DeviceIdType.MESH)

    local = []

    def load(src, dst):
        cp = pltpu.make_async_copy(src, dst, lsem.at[len(local)])
        cp.start()
        local.append(cp)
        return cp

    own = pl.ds(pl.multiple_of(tp * 1024, 1024), 1024)
    oth = pl.ds(pl.multiple_of(other * 1024, 1024), 1024)
    here, there = pl.ds(0, 1024), pl.ds(1024, 1024)

    def load2(a, b, rows, dst, to, w):
        return [load(a.at[rows], dst.at[to, pl.ds(0, w)]), load(b.at[rows], dst.at[to, pl.ds(w, w)])]

    c_tok = load(tok.at[0], tok_o)
    c_ld = [load(ld.at[h], ld_v.at[pl.ds(h, 1)]) for h in range(6)]
    c_gain = load(gain, gain_v)
    c_kv = load2(wrk, wrv, own, wkv, here, 384)

    lane1 = iota((1, 128), 1)
    m0 = jnp.where(lane1 < 64, 1.0, 0.0).astype(bf16)
    m1 = jnp.where(lane1 < 64, 0.0, 1.0).astype(bf16)
    wmask[0:C] = jnp.where(iota((C, C), 0) > iota((C, C), 1), 1.0, 0.0).astype(bf16)
    wmask[C:] = jnp.where(iota((C, C), 0) > iota((C, C), 1), 0.0, 1.0).astype(bf16)
    biasc[...] = jnp.where(iota((C, C), 0) >= iota((C, C), 1), 0.0, NEG)

    for cp in c_ld:
        cp.wait()
    raw = ld_v[...]
    rows48 = jnp.concatenate([raw[:, c * C:(c + 1) * C] for c in range(NC)], axis=0)
    rows48 = jnp.where(lax.rem(iota((48, C), 0), 8) < 6, rows48, 0.0)
    upper = jnp.where(iota((C, C), 0) <= iota((C, C), 1), 1.0, 0.0).astype(bf16)
    parts = jnp.concatenate(split3(rows48), axis=0).astype(bf16)
    summed = dot(parts, upper)
    lc = summed[0:48] + summed[48:96] + summed[96:144]
    lcrow[...] = lc
    sr, sl = lax.rem(iota((24, 1152), 0), 8), iota((24, 1152), 1)
    head_of = jnp.where(sl < 384, lax.div(sl, 64), lax.div(sl - 384, 128))
    sel = jnp.where(sr == head_of, 1.0, 0.0).astype(bf16)
    before = jnp.zeros((1, 384), f32)
    for c in range(NC):
        p3 = jnp.concatenate(split3(lc[c * 8:(c + 1) * 8]), axis=0).astype(bf16)
        cols = t_dot(p3, sel)
        lch[pl.ds(c * C, C)] = cols[:, 384:]
        el[pl.ds(c * C, C)] = cols[:, :384]
        last = cols[C - 1:C, :384]
        tots[c:c + 1] = last
        et[c:c + 1] = jnp.exp(before)
        before = before + last
    for p in range(3):
        l_a[p:p + 1] = before[:, p * 128:(p + 1) * 128]

    c_gain.wait()
    c_tok.wait()
    c_a = load2(wak, wav, own, wa, here, 128)
    c_q = load2(wrq, waq, own, wq, here, 384)
    g_o = gain_v[:, own]
    g_p = gain_v[:, oth]

    def scale_rows(src, r0, g):
        x = src[pl.ds(r0, 64)].astype(f32)
        sq = x * x
        part = sq[:, 0:128]
        for j in range(1, 8):
            part = part + sq[:, j * 128:(j + 1) * 128]
        return (x * g).astype(bf16), part

    def own_rows(i, carry):
        r0 = pl.multiple_of(i * 64, 64)
        s, part = scale_rows(tok_o, r0, g_o)
        sc_o[pl.ds(r0, 64)] = s
        ssq[pl.ds(r0, 64)] = part
        return carry

    lax.fori_loop(0, T // 64, own_rows, 0)

    pl.semaphore_wait(barrier, len(greet))

    t_cp = []
    for r in range(2):
        rows = pl.ds(r * HALF, HALF)
        cp = pltpu.make_async_remote_copy(
            src_ref=tok.at[0, rows], dst_ref=tok_p.at[rows], send_sem=tsem.at[r], recv_sem=trec.at[r],
            device_id=peer, device_id_type=pl.DeviceIdType.MESH)
        cp.start()
        t_cp.append(cp)
    w_cp = []
    for i, w in enumerate((wre, wao)):
        cp = pltpu.make_async_remote_copy(
            src_ref=w, dst_ref=wo.at[i, pl.ds(384, 384)], send_sem=wsem.at[i], recv_sem=wrec.at[i],
            device_id=peer, device_id_type=pl.DeviceIdType.MESH)
        cp.start()
        w_cp.append(cp)

    c_kv2 = load2(wrk, wrv, oth, wkv, there, 384)
    c_a2 = load2(wak, wav, oth, wa, there, 128)
    c_q2 = load2(wrq, waq, oth, wq, there, 384)
    c_small = [load(rgain, rgain_v), load(sink, sink_v)]
    c_wo = [load(wre, wo.at[0, pl.ds(0, 384)]), load(wao, wo.at[1, pl.ds(0, 384)])]

    def first_half(acc, w):
        for r in range(2):
            rows = pl.ds(r * HALF, HALF)
            acc[rows] = dot(sc_o[rows], w[here])

    def wait_all(cps):
        for cp in cps:
            cp.wait()

    wait_all(c_kv)
    first_half(acc_kv, wkv)
    wait_all(c_a)
    first_half(acc_a, wa)

    inv = [None, None]
    wait_all(c_kv2)
    for r in range(2):
        t_cp[r].wait_recv()

        def peer_rows(i, carry):
            r0 = pl.multiple_of(r * HALF + i * 64, 64)
            s, part = scale_rows(tok_p, r0, g_p)
            tok_p[pl.ds(r0, 64)] = s
            total = jnp.sum(ssq[pl.ds(r0, 64)] + part, axis=1, keepdims=True)
            ssq[pl.ds(r0, 64)] = jnp.broadcast_to(lax.rsqrt(total / D + EPS), (64, 128))
            return carry

        lax.fori_loop(0, HALF // 64, peer_rows, 0)
        rows = pl.ds(r * HALF, HALF)
        res = acc_kv[rows] + dot(tok_p[rows], wkv[there])
        kv[rows] = (res * ssq[rows, 0:1]).astype(bf16)

    lo = iota((64, 128), 1) < 64
    s_p = [jnp.zeros((64, 128), f32) for _ in range(3)]
    for c in range(NC):
        rows = pl.ds(c * C, C)
        tot = tots[c:c + 1]
        for p in range(3):
            cols = pl.ds(p * 128, 128)
            tp_ = tot[:, p * 128:(p + 1) * 128]
            lcp = el[rows, cols]
            kd = (kv[rows, cols].astype(f32) * jnp.exp(tp_ - lcp)).astype(bf16)
            m = t_dot(kd, kv[rows, pl.ds(384 + p * 128, 128)])
            comp = jnp.where(lo, m[0:64], m[64:128])
            st[c, p] = s_p[p].astype(bf16)
            s_p[p] = jnp.exp(tp_) * s_p[p] + comp
    for p in range(3):
        for q in range(4):
            st_a[q, p] = s_p[p][q * 16:(q + 1) * 16].astype(bf16)

    a_cp, al_cp = [], []

    def send(src, dst, ss, rs, who, group):
        cp = pltpu.make_async_remote_copy(
            src_ref=src, dst_ref=dst, send_sem=ss, recv_sem=rs, device_id=who,
            device_id_type=pl.DeviceIdType.MESH)
        cp.start()
        group.append(cp)

    def arrived(src, dst, ss, rs, who):
        pltpu.make_async_remote_copy(
            src_ref=src, dst_ref=dst, send_sem=ss, recv_sem=rs, device_id=who,
            device_id_type=pl.DeviceIdType.MESH).wait_recv()

    for d in range(1, 4):
        send(st_a.at[y_at[d]], buf_a.at[y], asem.at[d - 1], arec.at[y], at_y(d), a_cp)
        send(l_a, buf_al.at[y], alsem.at[d - 1], alrec.at[y], at_y(d), al_cp)
    buf_a[y] = st_a[y]
    buf_al[y] = l_a[...]

    wait_all(c_a2)
    for r in range(2):
        rows = pl.ds(r * HALF, HALF)
        res = acc_a[rows] + dot(tok_p[rows], wa[there])
        akv[pl.ds(C + r * HALF, HALF)] = (res * ssq[rows, 0:1]).astype(bf16)
    halo = pltpu.make_async_remote_copy(
        src_ref=akv.at[pl.ds(T, C)], dst_ref=akv.at[pl.ds(0, C)], send_sem=hsem, recv_sem=hrec,
        device_id=nxt, device_id_type=pl.DeviceIdType.MESH)
    halo.start()
    wait_all(c_q + c_q2)
    for r in range(2):
        rows = pl.ds(r * HALF, HALF)
        res = dot(jnp.concatenate([sc_o[rows], tok_p[rows]], axis=1), wq[...])
        res = res * (ssq[rows, 0:1] * 0.125)
        qb[rows] = res[:, :384].astype(bf16)
        for p in range(3):
            two = res[:, 384 + p * 128:384 + (p + 1) * 128]
            swapped = pltpu.roll(two, 64, 1) if p != 1 else two
            for j in range(2):
                h = 2 * p + j
                val = ((swapped if h in (1, 4) else two).astype(bf16)) * (m0 if h < 3 else m1)
                for b in range(3):
                    qs[r * 3 + b, pl.ds(h * C, C)] = val[b * C:(b + 1) * C]

    def spread(s):
        return jnp.concatenate([s * m0, s * m1], axis=0)

    def ret_chunk(i, carry):
        c = lax.rem(other * 3 + i, NC)
        rows = pl.ds(pl.multiple_of(c * C, C), C)
        past = et[pl.ds(c, 1)]
        lrows = lcrow[pl.ds(pl.multiple_of(c * 8, 8), 8)]
        for p in range(3):
            cols = pl.ds(p * 128, 128)
            q2, k2, v2 = qb[rows, cols], kv[rows, cols], kv[rows, pl.ds(384 + p * 128, 128)]
            ws = []
            for j, mj in enumerate((m0, m1)):
                h = 2 * p + j
                gap = lch[rows, pl.ds(h * 128, 128)] - lrows[h:h + 1] + biasc[...]
                ws.append((dot_t(q2 * mj, k2) * jnp.exp(gap)).astype(bf16))
            ex = jnp.exp(el[rows, cols])
            el[rows, cols] = ex * past[:, p * 128:(p + 1) * 128]
            ws.append((q2.astype(f32) * ex).astype(bf16))
            rhs = jnp.concatenate([v2 * m0, v2 * m1, spread(st[c, p])], axis=0)
            inner[rows, cols] = dot(jnp.concatenate(ws, axis=1), rhs)
        return carry


    for d in range(1, 4):
        arrived(st_a.at[0], buf_a.at[y_at[d]], asem.at[d - 1], arec.at[y_at[d]], at_y(d))
        arrived(l_a, buf_al.at[y_at[d]], alsem.at[d - 1], alrec.at[y_at[d]], at_y(d))
    b_cp, bl_cp = [], []
    for p in range(3):
        e = jnp.zeros((16, 128), f32)
        ltot = jnp.zeros((1, 128), f32)
        for yy in range(4):
            lyy = buf_al[yy][p:p + 1]
            e = jnp.exp(lyy) * e + buf_a[yy, p].astype(f32)
            ltot = ltot + lyy
        g_b[p] = e.astype(bf16)
        l_b[p:p + 1] = ltot
    for d in range(1, 8):
        send(g_b, buf_b.at[z], bsem.at[d - 1], brec.at[z], at_z(d), b_cp)
        send(l_b, buf_bl.at[z], blsem.at[d - 1], blrec.at[z], at_z(d), bl_cp)
    buf_b[z] = g_b[...]
    buf_bl[z] = l_b[...]

    wait_all(c_small)
    halo.wait_recv()
    sink_row = jnp.concatenate(
        [jnp.broadcast_to(sink_v[0:1, h:h + 1], (1, C)) for h in range(6)], axis=1)

    def att_block(i, half):
        n = half * 3 + i
        bandr = pl.ds(pl.multiple_of(n * C, C), 2 * C)
        edge = (n == 0) & (sp == 0)
        s = dot_t(akv[bandr, pl.ds(0, 128)], qs[n])
        is_own = iota((C, C), 0) <= iota((C, C), 1)
        ws, scale = [], []
        for h in range(6):
            hc = slice(h * C, (h + 1) * C)
            past = jnp.where(edge, NEG, s[:C, hc])
            v = jnp.where(is_own, s[C:, hc], past)
            sk = sink_row[:, hc]
            top = jnp.maximum(jnp.max(v, axis=0, keepdims=True), sk)
            e = jnp.exp(v - top)
            scale.append(1.0 / (jnp.sum(e, axis=0, keepdims=True) + jnp.exp(sk - top)))
            eb = e.astype(bf16)
            ws.append(jnp.concatenate([eb * wmask[0:C], eb * wmask[C:]], axis=0))
        o = t_dot(akv[bandr, pl.ds(128, 128)], jnp.concatenate(ws, axis=1))
        cols = pl.ds(pl.multiple_of(i * C, C), C)
        for h in range(6):
            r0 = 64 if h >= 3 else 0
            att[half, pl.ds(h * 64, 64), cols] = (
                o[r0:r0 + 64, h * C:(h + 1) * C] * scale[h]).astype(bf16)
        return half

    mine = pl.ds(pl.multiple_of(tp * HALF, HALF), HALF)
    theirs = pl.ds(pl.multiple_of(other * HALF, HALF), HALF)
    o_cp = []
    lax.fori_loop(0, 3, att_block, other)
    send(att.at[other], att_p, osem.at[0], orec.at[0], peer, o_cp)
    lax.fori_loop(0, 3, att_block, tp)
    lax.fori_loop(0, 4, ret_chunk, 0)

    for d in range(1, 8):
        arrived(g_b, buf_b.at[z_at[d]], bsem.at[d - 1], brec.at[z_at[d]], at_z(d))
        arrived(l_b, buf_bl.at[z_at[d]], blsem.at[d - 1], blrec.at[z_at[d]], at_z(d))
    for p in range(3):
        e = jnp.zeros((16, 128), f32)
        for zz in range(7):
            step = jnp.exp(buf_bl[zz][p:p + 1]) * e + buf_b[zz, p].astype(f32)
            e = jnp.where(zz < z, step, e)
        for yy in range(4):
            s_c[yy, p] = e.astype(bf16)
            e = jnp.exp(buf_al[yy][p:p + 1]) * e + buf_a[yy, p].astype(f32)
    c_cp = []
    for d in range(1, 4):
        send(s_c.at[y_at[d]], buf_c.at[y], csem.at[d - 1], crec.at[y], at_y(d), c_cp)
    buf_c[y] = s_c[y]

    lax.fori_loop(4, NC, ret_chunk, 0)

    wait_all(c_wo)
    w_cp[0].wait_recv()
    w_cp[1].wait_recv()
    o_cp[0].wait_recv()
    lhs = jnp.concatenate([att[tp], att_p[...]], axis=0)
    for j in range(4):
        cols = pl.ds(j * 512, 512)
        oacc[:, cols] = t_dot(lhs, wo[1, :, cols])

    for d in range(1, 4):
        arrived(s_c.at[0], buf_c.at[y_at[d]], csem.at[d - 1], crec.at[y_at[d]], at_y(d))
    big = [spread(jnp.concatenate([buf_c[q, p] for q in range(4)], axis=0)) for p in range(3)]
    ones_bd = jnp.where(
        lax.div(iota((128, 128), 0), 64) == lax.div(iota((128, 128), 1), 64), 1.0, 0.0).astype(bf16)

    def finish(rows):
        for p in range(3):
            cols = pl.ds(p * 128, 128)
            full = inner[rows, cols] + dot(qb[rows, cols], big[p]) * el[rows, cols]
            ms = dot((full * full).astype(bf16), ones_bd) * (1.0 / 64)
            ret[rows, cols] = (full * lax.rsqrt(ms + EPS) * rgain_v[cols].reshape(1, 128)).astype(bf16)

    finish(theirs)
    send(ret.at[theirs], ret_p, osem.at[1], orec.at[1], peer, o_cp)
    finish(mine)
    for j in range(4):
        cols = pl.ds(j * 512, 512)
        oacc[:, cols] += dot(ret[mine], wo[0, 0:384, cols])
    o_cp[1].wait_recv()
    for j in range(4):
        cols = pl.ds(j * 512, 512)
        out[0, :, cols] = (oacc[:, cols] + dot(ret_p[...], wo[0, 384:768, cols])).astype(bf16)

    for cp in t_cp + w_cp + a_cp + al_cp + b_cp + bl_cp + c_cp + o_cp + [halo]:
        cp.wait_send()


def shards(tokens, in_gain, ret_query, ret_key, ret_value, att_query, att_key, att_value,
           log_decay, ret_gain, sink_logit, retentive_exit_matrix, out_att):
    hbm = pl.BlockSpec(memory_space=pltpu.HBM)
    V = pltpu.VMEM
    DMA = pltpu.SemaphoreType.DMA
    scratch = [
        V((1, D), f32), V((384,), f32), V((1, 6), f32), V((8, T), f32),
        V((T, 1024), bf16), V((T, 1024), bf16), V((T, 1024), bf16), V((T, 128), f32),
        V((D, 768), bf16), V((D, 768), bf16), V((D, 256), bf16),
        V((T, 768), f32), V((T, 256), f32),
        V((T, 768), bf16), V((T, 384), bf16), V((T + C, 256), bf16), V((NC, 768, 128), bf16),
        V((48, 128), f32), V((T, 768), f32), V((T, 384), f32), V((8, 384), f32), V((8, 384), f32),
        V((NC, 3, 64, 128), bf16), V((T, 384), f32),
        V((2 * C, C), bf16), V((C, C), f32),
        V((4, 3, 16, 128), bf16), V((4, 3, 16, 128), bf16), V((8, 128), f32), V((4, 8, 128), f32),
        V((3, 16, 128), bf16), V((8, 3, 16, 128), bf16), V((8, 128), f32), V((8, 8, 128), f32),
        V((4, 3, 16, 128), bf16), V((4, 3, 16, 128), bf16),
        V((2, 768, D), bf16), V((2, 384, HALF), bf16), V((384, HALF), bf16), V((T, 384), bf16),
        V((HALF, 384), bf16), V((HALF, D), f32),
        DMA((24,)), DMA((2,)), DMA((2,)), DMA((2,)), DMA((2,)), DMA(()), DMA(()),
        DMA((3,)), DMA((4,)), DMA((3,)), DMA((4,)), DMA((7,)), DMA((8,)), DMA((7,)), DMA((8,)),
        DMA((3,)), DMA((4,)), DMA((2,)), DMA((2,)),
    ]
    return pl.pallas_call(
        kernel,
        out_shape=jax.ShapeDtypeStruct((1, HALF, D), bf16),
        in_specs=[hbm] * 13,
        out_specs=pl.BlockSpec(memory_space=pltpu.VMEM),
        scratch_shapes=scratch,
        compiler_params=pltpu.CompilerParams(
            collective_id=0, has_side_effects=True, vmem_limit_bytes=48 * 1024 * 1024),
    )(*(pltpu.with_memory_space_constraint(arg, pltpu.HBM) for arg in (
        tokens, in_gain.reshape(1, D), ret_query, ret_key, ret_value, att_query, att_key, att_value,
        jnp.transpose(log_decay, (1, 0, 2)), ret_gain, sink_logit.reshape(1, 6), retentive_exit_matrix, out_att,
    )))


def solution(mesh):
    placed = (
        P("fs", "sp", "tp"), P(), P(None, "tp"), P(None, "tp"), P(None, "tp"), P(None, "tp"),
        P(None, "tp"), P(None, "tp"), P("fs", "tp", "sp"), P("tp"), P("tp"), P("tp", None), P("tp", None),
    )
    return jax.shard_map(
        shards, mesh=mesh, in_specs=placed, out_specs=P("fs", ("sp", "tp"), None), check_vma=False)
```

```python
import functools

import jax
import jax.numpy as jnp
from jax import lax
from jax.experimental import pallas as pl
from jax.experimental.pallas import tpu as pltpu
from jax.sharding import PartitionSpec as P

EPS = 1e-06
D = 2048
T = 768
HALF = 384
C = 128
NC = 6
NEG = float("-inf")
f32 = jnp.float32
bf16 = jnp.bfloat16


def dot(a, b):
    return jnp.dot(a, b, preferred_element_type=f32)


def dot_t(a, b):
    return lax.dot_general(a, b, (((1,), (1,)), ((), ())), preferred_element_type=f32)


def t_dot(a, b):
    return lax.dot_general(a, b, (((0,), (0,)), ((), ())), preferred_element_type=f32)


def split3(x):
    a = x.astype(bf16).astype(f32)
    r = x - a
    b = r.astype(bf16).astype(f32)
    return a, b, (r - b).astype(bf16).astype(f32)


def iota(shape, dim):
    return lax.broadcasted_iota(jnp.int32, shape, dim)


def kernel(
    tok, gain, wrq, wrk, wrv, waq, wak, wav, ld, rgain, sink, wre, wao,
    out,
    gain_v, rgain_v, sink_v, ld_v,
    tok_o, tok_p, sc_o, ssq,
    wkv, wq, wa, acc_kv, acc_a,
    kv, qb, akv, qs,
    lcrow, exr, frow, lch, el, tots, st, inner, gcol,
    wmask, biasc,
    st_a, buf_a, l_a, buf_al, g_b, buf_b, l_b, buf_bl, s_c, buf_c,
    wo, att, att_p, ret, ret_p, oacc,
    lsem, tsem, trec, wsem, wrec, hsem, hrec,
    asem, arec, alsem, alrec, bsem, brec, blsem, blrec, csem, crec, osem, orec,
):
    sp = lax.axis_index("sp")
    tp = lax.axis_index("tp")
    y = lax.rem(sp, 4)
    z = lax.div(sp, 4)
    other = 1 - tp
    peer = {"tp": other}
    y_at = [lax.rem(y + d, 4) for d in range(4)]
    z_at = [lax.rem(z + d, 8) for d in range(8)]

    def at_y(d):
        return {"sp": z * 4 + y_at[d]}

    def at_z(d):
        return {"sp": z_at[d] * 4 + y}

    nxt = {"sp": lax.rem(sp + 1, 32)}
    prv = {"sp": lax.rem(sp + 31, 32)}

    barrier = pltpu.get_barrier_semaphore()
    greet = [peer] + [at_y(d) for d in range(1, 4)] + [at_z(d) for d in range(1, 8)] + [prv]
    for who in greet:
        pl.semaphore_signal(barrier, inc=1, device_id=who, device_id_type=pl.DeviceIdType.MESH)

    local = []

    def load(src, dst):
        cp = pltpu.make_async_copy(src, dst, lsem.at[len(local)])
        cp.start()
        local.append(cp)
        return cp

    own = pl.ds(pl.multiple_of(tp * 1024, 1024), 1024)
    oth = pl.ds(pl.multiple_of(other * 1024, 1024), 1024)
    here, there = pl.ds(0, 1024), pl.ds(1024, 1024)

    def load2(a, b, rows, dst, to, w):
        return [load(a.at[rows], dst.at[to, pl.ds(0, w)]), load(b.at[rows], dst.at[to, pl.ds(w, w)])]

    c_tok = load(tok.at[0], tok_o)
    c_ld = [load(ld.at[h], ld_v.at[pl.ds(h, 1)]) for h in range(6)]
    c_gain = load(gain, gain_v)

    lane1 = iota((1, 128), 1)
    m0 = jnp.where(lane1 < 64, 1.0, 0.0).astype(bf16)
    m1 = jnp.where(lane1 < 64, 0.0, 1.0).astype(bf16)
    wmask[0:C] = jnp.where(iota((C, C), 0) > iota((C, C), 1), 1.0, 0.0).astype(bf16)
    wmask[C:] = jnp.where(iota((C, C), 0) > iota((C, C), 1), 0.0, 1.0).astype(bf16)
    biasc[...] = jnp.where(iota((C, C), 0) <= iota((C, C), 1), 0.0, NEG)

    for cp in c_ld:
        cp.wait()
    raw = ld_v[...]
    rows48 = jnp.concatenate([raw[:, c * C:(c + 1) * C] for c in range(NC)], axis=0)
    rows48 = jnp.where(lax.rem(iota((48, C), 0), 8) < 6, rows48, 0.0)
    upper = jnp.where(iota((C, C), 0) <= iota((C, C), 1), 1.0, 0.0).astype(bf16)
    parts = jnp.concatenate(split3(rows48), axis=0).astype(bf16)
    summed = dot(parts, upper)
    lc = summed[0:48] + summed[48:96] + summed[96:144]
    lcrow[...] = lc
    sr, sl = lax.rem(iota((24, 1152), 0), 8), iota((24, 1152), 1)
    head_of = jnp.where(sl < 384, lax.div(sl, 64), lax.div(sl - 384, 128))
    sel = jnp.where(sr == head_of, 1.0, 0.0).astype(bf16)
    exr[...] = jnp.exp(lc)
    before = jnp.zeros((1, 384), f32)
    before8 = jnp.zeros((8, 1), f32)
    for c in range(NC):
        p3 = jnp.concatenate(split3(lc[c * 8:(c + 1) * 8]), axis=0).astype(bf16)
        cols = t_dot(p3, sel)
        lch[pl.ds(c * C, C)] = cols[:, 384:]
        el[pl.ds(c * C, C)] = cols[:, :384]
        last = cols[C - 1:C, :384]
        tots[c:c + 1] = last
        before = before + last
        lc8 = lc[c * 8:(c + 1) * 8]
        frow[c * 8:(c + 1) * 8] = jnp.exp(lc8 + before8)
        before8 = before8 + lc8[:, C - 1:C]
    for p in range(3):
        l_a[p:p + 1] = before[:, p * 128:(p + 1) * 128]

    c_gain.wait()
    c_tok.wait()
    c_kv = load2(wrk, wrv, own, wkv, here, 384)
    c_a = load2(wak, wav, own, wa, here, 128)
    c_q = load2(wrq, waq, own, wq, here, 384)
    g_o = gain_v[:, own]
    g_p = gain_v[:, oth]

    def scale_rows(src, r0, g):
        x = src[pl.ds(r0, 64)].astype(f32)
        sq = x * x
        part = sq[:, 0:128]
        for j in range(1, 8):
            part = part + sq[:, j * 128:(j + 1) * 128]
        return (x * g).astype(bf16), part

    def own_rows(i, carry):
        r0 = pl.multiple_of(i * 64, 64)
        s, part = scale_rows(tok_o, r0, g_o)
        sc_o[pl.ds(r0, 64)] = s
        ssq[pl.ds(r0, 64)] = part
        return carry

    lax.fori_loop(0, T // 64, own_rows, 0)

    pl.semaphore_wait(barrier, len(greet))

    t_cp = []
    for r in range(2):
        rows = pl.ds(r * HALF, HALF)
        cp = pltpu.make_async_remote_copy(
            src_ref=tok_o.at[rows], dst_ref=tok_p.at[rows], send_sem=tsem.at[r], recv_sem=trec.at[r],
            device_id=peer, device_id_type=pl.DeviceIdType.MESH)
        cp.start()
        t_cp.append(cp)
    c_kv2 = load2(wrk, wrv, oth, wkv, there, 384)
    c_a2 = load2(wak, wav, oth, wa, there, 128)
    c_q2 = load2(wrq, waq, oth, wq, there, 384)
    c_small = [load(rgain, rgain_v), load(sink, sink_v)]
    c_wo = [load(wre, wo.at[0, pl.ds(0, 384)]), load(wao, wo.at[1, pl.ds(0, 384)])]

    def first_half(acc, w):
        for r in range(2):
            rows = pl.ds(r * HALF, HALF)
            acc[rows] = dot(sc_o[rows], w[here])

    def wait_all(cps):
        for cp in cps:
            cp.wait()

    wait_all(c_kv)
    first_half(acc_kv, wkv)
    wait_all(c_a)
    first_half(acc_a, wa)

    inv = [None, None]
    wait_all(c_kv2)
    for r in range(2):
        t_cp[r].wait_recv()

        def peer_rows(i, carry):
            r0 = pl.multiple_of(r * HALF + i * 64, 64)
            s, part = scale_rows(tok_p, r0, g_p)
            tok_p[pl.ds(r0, 64)] = s
            total = jnp.sum(ssq[pl.ds(r0, 64)] + part, axis=1, keepdims=True)
            ssq[pl.ds(r0, 64)] = jnp.broadcast_to(lax.rsqrt(total / D + EPS), (64, 128))
            return carry

        lax.fori_loop(0, HALF // 64, peer_rows, 0)
        rows = pl.ds(r * HALF, HALF)
        res = acc_kv[rows] + dot(tok_p[rows], wkv[there])
        kv[rows] = (res * ssq[rows, 0:1]).astype(bf16)

    w_cp = []
    for i, w in enumerate((wre, wao)):
        cp = pltpu.make_async_remote_copy(
            src_ref=w, dst_ref=wo.at[i, pl.ds(384, 384)], send_sem=wsem.at[i], recv_sem=wrec.at[i],
            device_id=peer, device_id_type=pl.DeviceIdType.MESH)
        cp.start()
        w_cp.append(cp)

    lo = iota((64, 128), 1) < 64
    s_p = [jnp.zeros((64, 128), f32) for _ in range(3)]
    for c in range(NC):
        rows = pl.ds(c * C, C)
        tot = tots[c:c + 1]
        for p in range(3):
            cols = pl.ds(p * 128, 128)
            tp_ = tot[:, p * 128:(p + 1) * 128]
            lcp = el[rows, cols]
            kd = (kv[rows, cols].astype(f32) * jnp.exp(tp_ - lcp)).astype(bf16)
            m = t_dot(kv[rows, pl.ds(384 + p * 128, 128)], kd)
            comp = jnp.where(lo, m[0:64], m[64:128])
            st[c, p] = s_p[p].astype(bf16)
            s_p[p] = jnp.exp(tp_) * s_p[p] + comp
    for p in range(3):
        for q in range(4):
            st_a[q, p] = s_p[p][q * 16:(q + 1) * 16].astype(bf16)

    a_cp, al_cp = [], []

    def send(src, dst, ss, rs, who, group):
        cp = pltpu.make_async_remote_copy(
            src_ref=src, dst_ref=dst, send_sem=ss, recv_sem=rs, device_id=who,
            device_id_type=pl.DeviceIdType.MESH)
        cp.start()
        group.append(cp)

    def arrived(src, dst, ss, rs, who):
        pltpu.make_async_remote_copy(
            src_ref=src, dst_ref=dst, send_sem=ss, recv_sem=rs, device_id=who,
            device_id_type=pl.DeviceIdType.MESH).wait_recv()

    for d in range(1, 4):
        send(st_a.at[y_at[d]], buf_a.at[y], asem.at[d - 1], arec.at[y], at_y(d), a_cp)
        send(l_a, buf_al.at[y], alsem.at[d - 1], alrec.at[y], at_y(d), al_cp)
    buf_a[y] = st_a[y]
    buf_al[y] = l_a[...]

    wait_all(c_a2)
    for r in range(2):
        rows = pl.ds(r * HALF, HALF)
        res = acc_a[rows] + dot(tok_p[rows], wa[there])
        akv[pl.ds(C + r * HALF, HALF)] = (res * ssq[rows, 0:1]).astype(bf16)
    halo = pltpu.make_async_remote_copy(
        src_ref=akv.at[pl.ds(T, C)], dst_ref=akv.at[pl.ds(0, C)], send_sem=hsem, recv_sem=hrec,
        device_id=nxt, device_id_type=pl.DeviceIdType.MESH)
    halo.start()
    wait_all(c_q + c_q2)
    for r in range(2):
        rows = pl.ds(r * HALF, HALF)
        res = dot(jnp.concatenate([sc_o[rows], tok_p[rows]], axis=1), wq[...])
        res = res * (ssq[rows, 0:1] * 0.125)
        qb[rows] = res[:, :384].astype(bf16)
        for p in range(3):
            two = res[:, 384 + p * 128:384 + (p + 1) * 128]
            swapped = pltpu.roll(two, 64, 1) if p != 1 else two
            for j in range(2):
                h = 2 * p + j
                val = ((swapped if h in (1, 4) else two).astype(bf16)) * (m0 if h < 3 else m1)
                for b in range(3):
                    qs[r * 3 + b, pl.ds(h * C, C)] = val[b * C:(b + 1) * C]

    def spread(s):
        return jnp.concatenate([s * m0, s * m1], axis=0)

    def ret_pair(i, carry):
        todo = []
        for u in range(2):
            c = lax.rem(other * 3 + 2 * i + u, NC)
            half, lanes = lax.div(c, 3), pl.ds(pl.multiple_of(lax.rem(c, 3) * C, C), C)
            rows = pl.ds(pl.multiple_of(c * C, C), C)
            eight = pl.ds(pl.multiple_of(c * 8, 8), 8)
            for p in range(3):
                q2 = qb[rows, pl.ds(p * 128, 128)]
                s = dot_t(kv[rows, pl.ds(p * 128, 128)], jnp.concatenate([q2 * m0, q2 * m1], axis=0))
                todo.append((p, half, lanes, rows, lcrow[eight], exr[eight], s, dot_t(spread(st[c, p]), q2)))
        for p, half, lanes, rows, lrows, erows, s, past in todo:
            ws = []
            for j in range(2):
                h = 2 * p + j
                gap = lrows[h:h + 1] - lch[rows, pl.ds(h * 128, 128)] + biasc[...]
                ws.append((s[:, j * C:(j + 1) * C] * jnp.exp(gap)).astype(bf16))
            o = t_dot(kv[rows, pl.ds(384 + p * 128, 128)], jnp.concatenate(ws, axis=1))
            for j in range(2):
                h, r = 2 * p + j, slice(j * 64, (j + 1) * 64)
                inner[half, pl.ds(h * 64, 64), lanes] = o[r, j * C:(j + 1) * C] + past[r] * erows[h:h + 1]
        return carry

    for d in range(1, 4):
        arrived(st_a.at[0], buf_a.at[y_at[d]], asem.at[d - 1], arec.at[y_at[d]], at_y(d))
        arrived(l_a, buf_al.at[y_at[d]], alsem.at[d - 1], alrec.at[y_at[d]], at_y(d))
    b_cp, bl_cp = [], []
    for p in range(3):
        e = jnp.zeros((16, 128), f32)
        ltot = jnp.zeros((1, 128), f32)
        for yy in range(4):
            lyy = buf_al[yy][p:p + 1]
            e = jnp.exp(lyy) * e + buf_a[yy, p].astype(f32)
            ltot = ltot + lyy
        g_b[p] = e.astype(bf16)
        l_b[p:p + 1] = ltot
    for d in range(1, 8):
        send(g_b, buf_b.at[z], bsem.at[d - 1], brec.at[z], at_z(d), b_cp)
        send(l_b, buf_bl.at[z], blsem.at[d - 1], blrec.at[z], at_z(d), bl_cp)
    buf_b[z] = g_b[...]
    buf_bl[z] = l_b[...]

    lax.fori_loop(0, 2, ret_pair, 0)

    wait_all(c_small)
    halo.wait_recv()
    for p in range(3):
        g = jnp.broadcast_to(rgain_v[pl.ds(p * C, C)].reshape(1, C), (C, C))
        gcol[pl.ds(p * C, C)] = jnp.transpose(g)
    sink_row = jnp.concatenate(
        [jnp.broadcast_to(sink_v[0:1, h:h + 1], (1, C)) for h in range(6)], axis=1)

    def att_half(half):
        is_own = iota((C, C), 0) <= iota((C, C), 1)

        def scores(i):
            n = half * 3 + i
            return dot_t(akv[pl.ds(pl.multiple_of(n * C, C), 2 * C), pl.ds(0, 128)], qs[n])

        def block(i, s):
            n = half * 3 + i
            ws, scale = [], []
            for h in range(6):
                hc = slice(h * C, (h + 1) * C)
                past = s[:C, hc]
                if i == 0:
                    past = jnp.where((n == 0) & (sp == 0), NEG, past)
                v = jnp.where(is_own, s[C:, hc], past)
                sk = sink_row[:, hc]
                top = jnp.maximum(jnp.max(v, axis=0, keepdims=True), sk)
                e = jnp.exp(v - top)
                scale.append(1.0 / (jnp.sum(e, axis=0, keepdims=True) + jnp.exp(sk - top)))
                eb = e.astype(bf16)
                ws.append(jnp.concatenate([eb * wmask[0:C], eb * wmask[C:]], axis=0))
            bandr = pl.ds(pl.multiple_of(n * C, C), 2 * C)
            return scale, t_dot(akv[bandr, pl.ds(128, 128)], jnp.concatenate(ws, axis=1))

        ahead = scores(0)
        for i in range(3):
            s = ahead
            if i < 2:
                ahead = scores(i + 1)
            scale, o = block(i, s)
            for h in range(6):
                r0 = 64 if h >= 3 else 0
                att[half, pl.ds(h * 64, 64), pl.ds(i * C, C)] = (
                    o[r0:r0 + 64, h * C:(h + 1) * C] * scale[h]).astype(bf16)

    mine = pl.ds(pl.multiple_of(tp * HALF, HALF), HALF)
    theirs = pl.ds(pl.multiple_of(other * HALF, HALF), HALF)
    o_cp = []
    att_half(other)
    send(att.at[other], att_p, osem.at[0], orec.at[0], peer, o_cp)
    att_half(tp)

    for d in range(1, 8):
        arrived(g_b, buf_b.at[z_at[d]], bsem.at[d - 1], brec.at[z_at[d]], at_z(d))
        arrived(l_b, buf_bl.at[z_at[d]], blsem.at[d - 1], blrec.at[z_at[d]], at_z(d))
    for p in range(3):
        e = jnp.zeros((16, 128), f32)
        for zz in range(7):
            step = jnp.exp(buf_bl[zz][p:p + 1]) * e + buf_b[zz, p].astype(f32)
            e = jnp.where(zz < z, step, e)
        for yy in range(4):
            s_c[yy, p] = e.astype(bf16)
            e = jnp.exp(buf_al[yy][p:p + 1]) * e + buf_a[yy, p].astype(f32)
    c_cp = []
    for d in range(1, 4):
        send(s_c.at[y_at[d]], buf_c.at[y], csem.at[d - 1], crec.at[y], at_y(d), c_cp)
    buf_c[y] = s_c[y]

    ret_pair(2, 0)

    wait_all(c_wo)
    w_cp[0].wait_recv()
    w_cp[1].wait_recv()
    o_cp[0].wait_recv()
    lhs = jnp.concatenate([att[tp], att_p[...]], axis=0)
    for j in range(4):
        cols = pl.ds(j * 512, 512)
        oacc[:, cols] = t_dot(lhs, wo[1, :, cols])

    for d in range(1, 4):
        arrived(s_c.at[0], buf_c.at[y_at[d]], csem.at[d - 1], crec.at[y_at[d]], at_y(d))
    big = [spread(jnp.concatenate([buf_c[q, p] for q in range(4)], axis=0)) for p in range(3)]

    def finish(hf, rows):
        for p in range(3):
            car = dot_t(big[p], qb[rows, pl.ds(p * 128, 128)])
            for b in range(3):
                lanes = slice(b * C, (b + 1) * C)
                f8 = frow[pl.ds(pl.multiple_of((hf * 3 + b) * 8, 8), 8)]
                for j in range(2):
                    h = 2 * p + j
                    hr = pl.ds(h * 64, 64)
                    full = inner[hf, hr, pl.ds(b * C, C)] + car[j * 64:(j + 1) * 64, lanes] * f8[h:h + 1]
                    ms = jnp.sum(full * full, axis=0, keepdims=True) * (1.0 / 64)
                    ret[hf, hr, pl.ds(b * C, C)] = (full * lax.rsqrt(ms + EPS) * gcol[hr]).astype(bf16)

    finish(other, theirs)
    send(ret.at[other], ret_p, osem.at[1], orec.at[1], peer, o_cp)
    finish(tp, mine)
    for j in range(4):
        cols = pl.ds(j * 512, 512)
        oacc[:, cols] += t_dot(ret[tp], wo[0, 0:384, cols])
    o_cp[1].wait_recv()
    for j in range(4):
        cols = pl.ds(j * 512, 512)
        out[0, :, cols] = (oacc[:, cols] + t_dot(ret_p[...], wo[0, 384:768, cols])).astype(bf16)

    for cp in t_cp + w_cp + a_cp + al_cp + b_cp + bl_cp + c_cp + o_cp + [halo]:
        cp.wait_send()


def shards(tokens, in_gain, ret_query, ret_key, ret_value, att_query, att_key, att_value,
           log_decay, ret_gain, sink_logit, retentive_exit_matrix, out_att):
    hbm = pl.BlockSpec(memory_space=pltpu.HBM)
    V = pltpu.VMEM
    DMA = pltpu.SemaphoreType.DMA
    scratch = [
        V((1, D), f32), V((384,), f32), V((1, 6), f32), V((8, T), f32),
        V((T, 1024), bf16), V((T, 1024), bf16), V((T, 1024), bf16), V((T, 128), f32),
        V((D, 768), bf16), V((D, 768), bf16), V((D, 256), bf16),
        V((T, 768), f32), V((T, 256), f32),
        V((T, 768), bf16), V((T, 384), bf16), V((T + C, 256), bf16), V((NC, 768, 128), bf16),
        V((48, 128), f32), V((48, 128), f32), V((48, 128), f32), V((T, 768), f32), V((T, 384), f32), V((8, 384), f32),
        V((NC, 3, 64, 128), bf16), V((2, 384, HALF), f32), V((384, 128), f32),
        V((2 * C, C), bf16), V((C, C), f32),
        V((4, 3, 16, 128), bf16), V((4, 3, 16, 128), bf16), V((8, 128), f32), V((4, 8, 128), f32),
        V((3, 16, 128), bf16), V((8, 3, 16, 128), bf16), V((8, 128), f32), V((8, 8, 128), f32),
        V((4, 3, 16, 128), bf16), V((4, 3, 16, 128), bf16),
        V((2, 768, D), bf16), V((2, 384, HALF), bf16), V((384, HALF), bf16), V((2, 384, HALF), bf16),
        V((384, HALF), bf16), V((HALF, D), f32),
        DMA((24,)), DMA((2,)), DMA((2,)), DMA((2,)), DMA((2,)), DMA(()), DMA(()),
        DMA((3,)), DMA((4,)), DMA((3,)), DMA((4,)), DMA((7,)), DMA((8,)), DMA((7,)), DMA((8,)),
        DMA((3,)), DMA((4,)), DMA((2,)), DMA((2,)),
    ]
    return pl.pallas_call(
        kernel,
        out_shape=jax.ShapeDtypeStruct((1, HALF, D), bf16),
        in_specs=[hbm] * 13,
        out_specs=pl.BlockSpec(memory_space=pltpu.VMEM),
        scratch_shapes=scratch,
        compiler_params=pltpu.CompilerParams(
            collective_id=0, has_side_effects=True, vmem_limit_bytes=48 * 1024 * 1024),
    )(*(pltpu.with_memory_space_constraint(arg, pltpu.HBM) for arg in (
        tokens, in_gain.reshape(1, D), ret_query, ret_key, ret_value, att_query, att_key, att_value,
        jnp.transpose(log_decay, (1, 0, 2)), ret_gain, sink_logit.reshape(1, 6), retentive_exit_matrix, out_att,
    )))


def solution(mesh):
    placed = (
        P("fs", "sp", "tp"), P(), P(None, "tp"), P(None, "tp"), P(None, "tp"), P(None, "tp"),
        P(None, "tp"), P(None, "tp"), P("fs", "tp", "sp"), P("tp"), P("tp"), P("tp", None), P("tp", None),
    )
    return jax.shard_map(
        shards, mesh=mesh, in_specs=placed, out_specs=P("fs", ("sp", "tp"), None), check_vma=False)
```

```python
import functools

import jax
import jax.numpy as jnp
from jax import lax
from jax.experimental import pallas as pl
from jax.experimental.pallas import tpu as pltpu
from jax.sharding import PartitionSpec as P

EPS = 1e-06
D = 2048
T = 768
HALF = 384
C = 128
NC = 6
NEG = float("-inf")
f32 = jnp.float32
bf16 = jnp.bfloat16


def dot(a, b):
    return jnp.dot(a, b, preferred_element_type=f32)


def dot_t(a, b):
    return lax.dot_general(a, b, (((1,), (1,)), ((), ())), preferred_element_type=f32)


def t_dot(a, b):
    return lax.dot_general(a, b, (((0,), (0,)), ((), ())), preferred_element_type=f32)


def split3(x):
    a = x.astype(bf16).astype(f32)
    r = x - a
    b = r.astype(bf16).astype(f32)
    return a, b, (r - b).astype(bf16).astype(f32)


def iota(shape, dim):
    return lax.broadcasted_iota(jnp.int32, shape, dim)


def kernel(
    tok, gain, wrq, wrk, wrv, waq, wak, wav, ld, rgain, sink, wre, wao,
    out,
    gain_v, rgain_v, sink_v, ld_v,
    tok_o, tok_p, sc_o, ssq,
    wkv, wq, wa, acc_kv, acc_a,
    kv, qb, akv, qs,
    lcrow, exr, frow, lch, el, tots, st, inner, gcol,
    wmask, biasc,
    st_a, buf_a, l_a, buf_al, g_b, buf_b, l_b, buf_bl, s_c, buf_c,
    wo, att, att_p, ret, ret_p, oacc,
    lsem, tsem, trec, wsem, wrec, hsem, hrec,
    asem, arec, alsem, alrec, bsem, brec, blsem, blrec, csem, crec, osem, orec,
):
    sp = lax.axis_index("sp")
    tp = lax.axis_index("tp")
    y = lax.rem(sp, 4)
    z = lax.div(sp, 4)
    other = 1 - tp
    peer = {"tp": other}
    y_at = [lax.rem(y + d, 4) for d in range(4)]
    z_at = [lax.rem(z + d, 8) for d in range(8)]

    def at_y(d):
        return {"sp": z * 4 + y_at[d]}

    def at_z(d):
        return {"sp": z_at[d] * 4 + y}

    nxt = {"sp": lax.rem(sp + 1, 32)}
    prv = {"sp": lax.rem(sp + 31, 32)}

    barrier = pltpu.get_barrier_semaphore()
    greet = [peer] + [at_y(d) for d in range(1, 4)] + [at_z(d) for d in range(1, 8)] + [prv]
    for who in greet:
        pl.semaphore_signal(barrier, inc=1, device_id=who, device_id_type=pl.DeviceIdType.MESH)

    local = []

    def load(src, dst):
        cp = pltpu.make_async_copy(src, dst, lsem.at[len(local)])
        cp.start()
        local.append(cp)
        return cp

    own = pl.ds(pl.multiple_of(tp * 1024, 1024), 1024)
    oth = pl.ds(pl.multiple_of(other * 1024, 1024), 1024)
    here, there = pl.ds(0, 1024), pl.ds(1024, 1024)

    def load2(a, b, rows, dst, to, w):
        return [load(a.at[rows], dst.at[to, pl.ds(0, w)]), load(b.at[rows], dst.at[to, pl.ds(w, w)])]

    c_tok = load(tok.at[0], tok_o)
    c_ld = [load(ld.at[h], ld_v.at[pl.ds(h, 1)]) for h in range(6)]
    c_gain = load(gain, gain_v)

    lane1 = iota((1, 128), 1)
    m0 = jnp.where(lane1 < 64, 1.0, 0.0).astype(bf16)
    m1 = jnp.where(lane1 < 64, 0.0, 1.0).astype(bf16)
    wmask[0:C] = jnp.where(iota((C, C), 0) > iota((C, C), 1), 1.0, 0.0).astype(bf16)
    wmask[C:] = jnp.where(iota((C, C), 0) > iota((C, C), 1), 0.0, 1.0).astype(bf16)
    biasc[...] = jnp.where(iota((C, C), 0) <= iota((C, C), 1), 0.0, NEG)

    for cp in c_ld:
        cp.wait()
    raw = ld_v[...]
    rows48 = jnp.concatenate([raw[:, c * C:(c + 1) * C] for c in range(NC)], axis=0)
    rows48 = jnp.where(lax.rem(iota((48, C), 0), 8) < 6, rows48, 0.0)
    upper = jnp.where(iota((C, C), 0) <= iota((C, C), 1), 1.0, 0.0).astype(bf16)
    parts = jnp.concatenate(split3(rows48), axis=0).astype(bf16)
    summed = dot(parts, upper)
    lc = summed[0:48] + summed[48:96] + summed[96:144]
    lcrow[...] = lc
    sr, sl = lax.rem(iota((24, 1152), 0), 8), iota((24, 1152), 1)
    head_of = jnp.where(sl < 384, lax.div(sl, 64), lax.div(sl - 384, 128))
    sel = jnp.where(sr == head_of, 1.0, 0.0).astype(bf16)
    exr[...] = jnp.exp(lc)
    before = jnp.zeros((1, 384), f32)
    before8 = jnp.zeros((8, 1), f32)
    for c in range(NC):
        p3 = jnp.concatenate(split3(lc[c * 8:(c + 1) * 8]), axis=0).astype(bf16)
        cols = t_dot(p3, sel)
        lch[pl.ds(c * C, C)] = cols[:, 384:]
        el[pl.ds(c * C, C)] = cols[:, :384]
        last = cols[C - 1:C, :384]
        tots[c:c + 1] = last
        before = before + last
        lc8 = lc[c * 8:(c + 1) * 8]
        frow[c * 8:(c + 1) * 8] = jnp.exp(lc8 + before8)
        before8 = before8 + lc8[:, C - 1:C]
    l_a[...] = jnp.zeros((8, 128), f32)
    for p in range(3):
        l_a[p:p + 1] = before[:, p * 128:(p + 1) * 128]

    c_gain.wait()
    c_tok.wait()
    c_kv = load2(wrk, wrv, own, wkv, here, 384)
    c_a = load2(wak, wav, own, wa, here, 128)
    c_kv2 = load2(wrk, wrv, oth, wkv, there, 384)
    c_a2 = load2(wak, wav, oth, wa, there, 128)
    c_q = load2(wrq, waq, own, wq, here, 384)
    c_q2 = load2(wrq, waq, oth, wq, there, 384)
    g_o = gain_v[:, own]
    g_p = gain_v[:, oth]

    def scale_rows(src, r0, g):
        x = src[pl.ds(r0, 64)].astype(f32)
        sq = x * x
        part = sq[:, 0:128]
        for j in range(1, 8):
            part = part + sq[:, j * 128:(j + 1) * 128]
        return (x * g).astype(bf16), part

    def own_rows(i, carry):
        r0 = pl.multiple_of(i * 64, 64)
        s, part = scale_rows(tok_o, r0, g_o)
        sc_o[pl.ds(r0, 64)] = s
        ssq[pl.ds(r0, 64)] = part
        return carry

    lax.fori_loop(0, T // 64, own_rows, 0)

    pl.semaphore_wait(barrier, len(greet))

    t_cp = []
    for r in range(2):
        rows = pl.ds(r * HALF, HALF)
        cp = pltpu.make_async_remote_copy(
            src_ref=tok_o.at[rows], dst_ref=tok_p.at[rows], send_sem=tsem.at[r], recv_sem=trec.at[r],
            device_id=peer, device_id_type=pl.DeviceIdType.MESH)
        cp.start()
        t_cp.append(cp)
    a_cp, al_cp, b_cp, bl_cp = [], [], [], []

    def send(src, dst, ss, rs, who, group):
        cp = pltpu.make_async_remote_copy(
            src_ref=src, dst_ref=dst, send_sem=ss, recv_sem=rs, device_id=who,
            device_id_type=pl.DeviceIdType.MESH)
        cp.start()
        group.append(cp)

    def arrived(src, dst, ss, rs, who):
        pltpu.make_async_remote_copy(
            src_ref=src, dst_ref=dst, send_sem=ss, recv_sem=rs, device_id=who,
            device_id_type=pl.DeviceIdType.MESH).wait_recv()

    for d in range(1, 4):
        send(l_a, buf_al.at[y], alsem.at[d - 1], alrec.at[y], at_y(d), al_cp)
    buf_al[y] = l_a[...]

    def first_half(acc, w):
        for r in range(2):
            rows = pl.ds(r * HALF, HALF)
            acc[rows] = dot(sc_o[rows], w[here])

    def wait_all(cps):
        for cp in cps:
            cp.wait()

    wait_all(c_kv)
    first_half(acc_kv, wkv)
    wait_all(c_a)
    first_half(acc_a, wa)

    c_small = [load(rgain, rgain_v), load(sink, sink_v)]
    c_wo = [load(wre, wo.at[0, pl.ds(0, 384)]), load(wao, wo.at[1, pl.ds(0, 384)])]

    wait_all(c_kv2)
    for r in range(2):
        t_cp[r].wait_recv()

        def peer_rows(i, carry):
            r0 = pl.multiple_of(r * HALF + i * 64, 64)
            s, part = scale_rows(tok_p, r0, g_p)
            tok_p[pl.ds(r0, 64)] = s
            total = jnp.sum(ssq[pl.ds(r0, 64)] + part, axis=1, keepdims=True)
            ssq[pl.ds(r0, 64)] = jnp.broadcast_to(lax.rsqrt(total / D + EPS), (64, 128))
            return carry

        lax.fori_loop(0, HALF // 64, peer_rows, 0)
        rows = pl.ds(r * HALF, HALF)
        res = acc_kv[rows] + dot(tok_p[rows], wkv[there])
        kv[rows] = (res * ssq[rows, 0:1]).astype(bf16)

    for d in range(1, 4):
        arrived(l_a, buf_al.at[y_at[d]], alsem.at[d - 1], alrec.at[y_at[d]], at_y(d))
    l_b[...] = buf_al[0] + buf_al[1] + buf_al[2] + buf_al[3]
    for d in range(1, 8):
        send(l_b, buf_bl.at[z], blsem.at[d - 1], blrec.at[z], at_z(d), bl_cp)
    buf_bl[z] = l_b[...]

    lo = iota((64, 128), 1) < 64
    s_p = [jnp.zeros((64, 128), f32) for _ in range(3)]
    for c in range(NC):
        rows = pl.ds(c * C, C)
        tot = tots[c:c + 1]
        for p in range(3):
            cols = pl.ds(p * 128, 128)
            tp_ = tot[:, p * 128:(p + 1) * 128]
            lcp = el[rows, cols]
            kd = (kv[rows, cols].astype(f32) * jnp.exp(tp_ - lcp)).astype(bf16)
            m = t_dot(kv[rows, pl.ds(384 + p * 128, 128)], kd)
            comp = jnp.where(lo, m[0:64], m[64:128])
            st[c, p] = s_p[p].astype(bf16)
            s_p[p] = jnp.exp(tp_) * s_p[p] + comp
    for p in range(3):
        for q in range(4):
            st_a[q, p] = s_p[p][q * 16:(q + 1) * 16].astype(bf16)

    for d in range(1, 4):
        send(st_a.at[y_at[d]], buf_a.at[y], asem.at[d - 1], arec.at[y], at_y(d), a_cp)
    buf_a[y] = st_a[y]

    w_cp = []
    for i, w in enumerate((wre, wao)):
        cp = pltpu.make_async_remote_copy(
            src_ref=w, dst_ref=wo.at[i, pl.ds(384, 384)], send_sem=wsem.at[i], recv_sem=wrec.at[i],
            device_id=peer, device_id_type=pl.DeviceIdType.MESH)
        cp.start()
        w_cp.append(cp)

    wait_all(c_a2)
    for r in range(2):
        rows = pl.ds(r * HALF, HALF)
        res = acc_a[rows] + dot(tok_p[rows], wa[there])
        akv[pl.ds(C + r * HALF, HALF)] = (res * ssq[rows, 0:1]).astype(bf16)
    halo = pltpu.make_async_remote_copy(
        src_ref=akv.at[pl.ds(T, C)], dst_ref=akv.at[pl.ds(0, C)], send_sem=hsem, recv_sem=hrec,
        device_id=nxt, device_id_type=pl.DeviceIdType.MESH)
    halo.start()
    wait_all(c_q + c_q2)
    for r in range(2):
        rows = pl.ds(r * HALF, HALF)
        res = dot(jnp.concatenate([sc_o[rows], tok_p[rows]], axis=1), wq[...])
        res = res * (ssq[rows, 0:1] * 0.125)
        qb[rows] = res[:, :384].astype(bf16)
        for p in range(3):
            two = res[:, 384 + p * 128:384 + (p + 1) * 128]
            swapped = pltpu.roll(two, 64, 1) if p != 1 else two
            for j in range(2):
                h = 2 * p + j
                val = ((swapped if h in (1, 4) else two).astype(bf16)) * (m0 if h < 3 else m1)
                for b in range(3):
                    qs[r * 3 + b, pl.ds(h * C, C)] = val[b * C:(b + 1) * C]

    def spread(s):
        return jnp.concatenate([s * m0, s * m1], axis=0)

    def ret_pair(i, carry):
        todo = []
        for u in range(2):
            c = lax.rem(other * 3 + 2 * i + u, NC)
            half, lanes = lax.div(c, 3), pl.ds(pl.multiple_of(lax.rem(c, 3) * C, C), C)
            rows = pl.ds(pl.multiple_of(c * C, C), C)
            eight = pl.ds(pl.multiple_of(c * 8, 8), 8)
            for p in range(3):
                q2 = qb[rows, pl.ds(p * 128, 128)]
                s = dot_t(kv[rows, pl.ds(p * 128, 128)], jnp.concatenate([q2 * m0, q2 * m1], axis=0))
                todo.append((p, half, lanes, rows, lcrow[eight], exr[eight], s, dot_t(spread(st[c, p]), q2)))
        for p, half, lanes, rows, lrows, erows, s, past in todo:
            ws = []
            for j in range(2):
                h = 2 * p + j
                gap = lrows[h:h + 1] - lch[rows, pl.ds(h * 128, 128)] + biasc[...]
                ws.append((s[:, j * C:(j + 1) * C] * jnp.exp(gap)).astype(bf16))
            o = t_dot(kv[rows, pl.ds(384 + p * 128, 128)], jnp.concatenate(ws, axis=1))
            for j in range(2):
                h, r = 2 * p + j, slice(j * 64, (j + 1) * 64)
                inner[half, pl.ds(h * 64, 64), lanes] = o[r, j * C:(j + 1) * C] + past[r] * erows[h:h + 1]
        return carry

    for d in range(1, 4):
        arrived(st_a.at[0], buf_a.at[y_at[d]], asem.at[d - 1], arec.at[y_at[d]], at_y(d))
    for p in range(3):
        e = jnp.zeros((16, 128), f32)
        for yy in range(4):
            lyy = buf_al[yy][p:p + 1]
            e = jnp.exp(lyy) * e + buf_a[yy, p].astype(f32)
        g_b[p] = e.astype(bf16)
    for d in range(1, 8):
        send(g_b, buf_b.at[z], bsem.at[d - 1], brec.at[z], at_z(d), b_cp)
    buf_b[z] = g_b[...]

    lax.fori_loop(0, 2, ret_pair, 0)

    wait_all(c_small)
    halo.wait_recv()
    for p in range(3):
        g = jnp.broadcast_to(rgain_v[pl.ds(p * C, C)].reshape(1, C), (C, C))
        gcol[pl.ds(p * C, C)] = jnp.transpose(g)
    sink_row = jnp.concatenate(
        [jnp.broadcast_to(sink_v[0:1, h:h + 1], (1, C)) for h in range(6)], axis=1)

    def att_half(half):
        is_own = iota((C, C), 0) <= iota((C, C), 1)

        def scores(i):
            n = half * 3 + i
            return dot_t(akv[pl.ds(pl.multiple_of(n * C, C), 2 * C), pl.ds(0, 128)], qs[n])

        def block(i, s):
            n = half * 3 + i
            ws, scale = [], []
            for h in range(6):
                hc = slice(h * C, (h + 1) * C)
                past = s[:C, hc]
                if i == 0:
                    past = jnp.where((n == 0) & (sp == 0), NEG, past)
                v = jnp.where(is_own, s[C:, hc], past)
                sk = sink_row[:, hc]
                top = jnp.maximum(jnp.max(v, axis=0, keepdims=True), sk)
                e = jnp.exp(v - top)
                scale.append(1.0 / (jnp.sum(e, axis=0, keepdims=True) + jnp.exp(sk - top)))
                eb = e.astype(bf16)
                ws.append(jnp.concatenate([eb * wmask[0:C], eb * wmask[C:]], axis=0))
            bandr = pl.ds(pl.multiple_of(n * C, C), 2 * C)
            return scale, t_dot(akv[bandr, pl.ds(128, 128)], jnp.concatenate(ws, axis=1))

        ahead = scores(0)
        for i in range(3):
            s = ahead
            if i < 2:
                ahead = scores(i + 1)
            scale, o = block(i, s)
            for h in range(6):
                r0 = 64 if h >= 3 else 0
                att[half, pl.ds(h * 64, 64), pl.ds(i * C, C)] = (
                    o[r0:r0 + 64, h * C:(h + 1) * C] * scale[h]).astype(bf16)

    mine = pl.ds(pl.multiple_of(tp * HALF, HALF), HALF)
    theirs = pl.ds(pl.multiple_of(other * HALF, HALF), HALF)
    o_cp = []
    att_half(other)
    send(att.at[other], att_p, osem.at[0], orec.at[0], peer, o_cp)
    att_half(tp)

    for d in range(1, 8):
        arrived(g_b, buf_b.at[z_at[d]], bsem.at[d - 1], brec.at[z_at[d]], at_z(d))
        arrived(l_b, buf_bl.at[z_at[d]], blsem.at[d - 1], blrec.at[z_at[d]], at_z(d))
    for p in range(3):
        e = jnp.zeros((16, 128), f32)
        for zz in range(7):
            step = jnp.exp(buf_bl[zz][p:p + 1]) * e + buf_b[zz, p].astype(f32)
            e = jnp.where(zz < z, step, e)
        for yy in range(4):
            s_c[yy, p] = e.astype(bf16)
            e = jnp.exp(buf_al[yy][p:p + 1]) * e + buf_a[yy, p].astype(f32)
    c_cp = []
    for d in range(1, 4):
        send(s_c.at[y_at[d]], buf_c.at[y], csem.at[d - 1], crec.at[y], at_y(d), c_cp)
    buf_c[y] = s_c[y]

    ret_pair(2, 0)

    wait_all(c_wo)
    w_cp[0].wait_recv()
    w_cp[1].wait_recv()
    o_cp[0].wait_recv()
    lhs = jnp.concatenate([att[tp], att_p[...]], axis=0)
    for j in range(4):
        cols = pl.ds(j * 512, 512)
        oacc[:, cols] = t_dot(lhs, wo[1, :, cols])

    for d in range(1, 4):
        arrived(s_c.at[0], buf_c.at[y_at[d]], csem.at[d - 1], crec.at[y_at[d]], at_y(d))
    big = [spread(jnp.concatenate([buf_c[q, p] for q in range(4)], axis=0)) for p in range(3)]

    def finish(hf, rows):
        for p in range(3):
            car = dot_t(big[p], qb[rows, pl.ds(p * 128, 128)])
            for b in range(3):
                lanes = slice(b * C, (b + 1) * C)
                f8 = frow[pl.ds(pl.multiple_of((hf * 3 + b) * 8, 8), 8)]
                for j in range(2):
                    h = 2 * p + j
                    hr = pl.ds(h * 64, 64)
                    full = inner[hf, hr, pl.ds(b * C, C)] + car[j * 64:(j + 1) * 64, lanes] * f8[h:h + 1]
                    ms = jnp.sum(full * full, axis=0, keepdims=True) * (1.0 / 64)
                    ret[hf, hr, pl.ds(b * C, C)] = (full * lax.rsqrt(ms + EPS) * gcol[hr]).astype(bf16)

    finish(other, theirs)
    send(ret.at[other], ret_p, osem.at[1], orec.at[1], peer, o_cp)
    finish(tp, mine)
    for j in range(4):
        cols = pl.ds(j * 512, 512)
        oacc[:, cols] += t_dot(ret[tp], wo[0, 0:384, cols])
    o_cp[1].wait_recv()
    for j in range(4):
        cols = pl.ds(j * 512, 512)
        out[0, :, cols] = (oacc[:, cols] + t_dot(ret_p[...], wo[0, 384:768, cols])).astype(bf16)

    for cp in t_cp + w_cp + a_cp + al_cp + b_cp + bl_cp + c_cp + o_cp + [halo]:
        cp.wait_send()


def shards(tokens, in_gain, ret_query, ret_key, ret_value, att_query, att_key, att_value,
           log_decay, ret_gain, sink_logit, retentive_exit_matrix, out_att):
    hbm = pl.BlockSpec(memory_space=pltpu.HBM)
    V = pltpu.VMEM
    DMA = pltpu.SemaphoreType.DMA
    scratch = [
        V((1, D), f32), V((384,), f32), V((1, 6), f32), V((8, T), f32),
        V((T, 1024), bf16), V((T, 1024), bf16), V((T, 1024), bf16), V((T, 128), f32),
        V((D, 768), bf16), V((D, 768), bf16), V((D, 256), bf16),
        V((T, 768), f32), V((T, 256), f32),
        V((T, 768), bf16), V((T, 384), bf16), V((T + C, 256), bf16), V((NC, 768, 128), bf16),
        V((48, 128), f32), V((48, 128), f32), V((48, 128), f32), V((T, 768), f32), V((T, 384), f32), V((8, 384), f32),
        V((NC, 3, 64, 128), bf16), V((2, 384, HALF), f32), V((384, 128), f32),
        V((2 * C, C), bf16), V((C, C), f32),
        V((4, 3, 16, 128), bf16), V((4, 3, 16, 128), bf16), V((8, 128), f32), V((4, 8, 128), f32),
        V((3, 16, 128), bf16), V((8, 3, 16, 128), bf16), V((8, 128), f32), V((8, 8, 128), f32),
        V((4, 3, 16, 128), bf16), V((4, 3, 16, 128), bf16),
        V((2, 768, D), bf16), V((2, 384, HALF), bf16), V((384, HALF), bf16), V((2, 384, HALF), bf16),
        V((384, HALF), bf16), V((HALF, D), f32),
        DMA((24,)), DMA((2,)), DMA((2,)), DMA((2,)), DMA((2,)), DMA(()), DMA(()),
        DMA((3,)), DMA((4,)), DMA((3,)), DMA((4,)), DMA((7,)), DMA((8,)), DMA((7,)), DMA((8,)),
        DMA((3,)), DMA((4,)), DMA((2,)), DMA((2,)),
    ]
    return pl.pallas_call(
        kernel,
        out_shape=jax.ShapeDtypeStruct((1, HALF, D), bf16),
        in_specs=[hbm] * 13,
        out_specs=pl.BlockSpec(memory_space=pltpu.VMEM),
        scratch_shapes=scratch,
        compiler_params=pltpu.CompilerParams(
            collective_id=0, has_side_effects=True, vmem_limit_bytes=48 * 1024 * 1024),
    )(*(pltpu.with_memory_space_constraint(arg, pltpu.HBM) for arg in (
        tokens, in_gain.reshape(1, D), ret_query, ret_key, ret_value, att_query, att_key, att_value,
        jnp.transpose(log_decay, (1, 0, 2)), ret_gain, sink_logit.reshape(1, 6), retentive_exit_matrix, out_att,
    )))


def solution(mesh):
    placed = (
        P("fs", "sp", "tp"), P(), P(None, "tp"), P(None, "tp"), P(None, "tp"), P(None, "tp"),
        P(None, "tp"), P(None, "tp"), P("fs", "tp", "sp"), P("tp"), P("tp"), P("tp", None), P("tp", None),
    )
    return jax.shard_map(
        shards, mesh=mesh, in_specs=placed, out_specs=P("fs", ("sp", "tp"), None), check_vma=False)
```

```python
import functools

import jax
import jax.numpy as jnp
from jax import lax
from jax.experimental import pallas as pl
from jax.experimental.pallas import tpu as pltpu
from jax.sharding import PartitionSpec as P

EPS = 1e-06
D = 2048
T = 768
HALF = 384
C = 128
NC = 6
NEG = float("-inf")
f32 = jnp.float32
bf16 = jnp.bfloat16


def dot(a, b):
    return jnp.dot(a, b, preferred_element_type=f32)


def dot_t(a, b):
    return lax.dot_general(a, b, (((1,), (1,)), ((), ())), preferred_element_type=f32)


def t_dot(a, b):
    return lax.dot_general(a, b, (((0,), (0,)), ((), ())), preferred_element_type=f32)


def split3(x):
    a = x.astype(bf16).astype(f32)
    r = x - a
    b = r.astype(bf16).astype(f32)
    return a, b, (r - b).astype(bf16).astype(f32)


def iota(shape, dim):
    return lax.broadcasted_iota(jnp.int32, shape, dim)


def kernel(
    tok, gain, wrq, wrk, wrv, waq, wak, wav, ld, rgain, sink, wre, wao,
    out,
    gain_v, rgain_v, sink_v, ld_v,
    tok_o, tok_p, sc_o, ssq,
    wkv, wq, wa, acc_kv, acc_a,
    kv, qb, akv, qs,
    lcrow, exr, frow, lch, el, tots, st, inner, gcol,
    wmask, biasc,
    st_a, buf_a, l_a, buf_al, g_b, buf_b, l_b, buf_bl, s_c, buf_c,
    wo, att, att_p, ret, oacc, in_p, q_p, frow_p, gcol_p,
    lsem, tsem, trec, wsem, wrec, hsem, hrec,
    asem, arec, alsem, alrec, bsem, brec, blsem, blrec, csem, crec, osem, orec, xsem, xrec,
):
    sp = lax.axis_index("sp")
    tp = lax.axis_index("tp")
    y = lax.rem(sp, 4)
    z = lax.div(sp, 4)
    other = 1 - tp
    peer = {"tp": other}
    y_at = [lax.rem(y + d, 4) for d in range(4)]
    z_at = [lax.rem(z + d, 8) for d in range(8)]

    def at_y(d):
        return {"sp": z * 4 + y_at[d]}

    def at_z(d):
        return {"sp": z_at[d] * 4 + y}

    def across_y(d):
        return {"sp": z * 4 + y_at[d], "tp": other}

    nxt = {"sp": lax.rem(sp + 1, 32)}
    prv = {"sp": lax.rem(sp + 31, 32)}

    barrier = pltpu.get_barrier_semaphore()
    greet = [peer] + [at_y(d) for d in range(1, 4)] + [across_y(d) for d in range(1, 4)] + [at_z(d) for d in range(1, 8)] + [prv]
    for who in greet:
        pl.semaphore_signal(barrier, inc=1, device_id=who, device_id_type=pl.DeviceIdType.MESH)

    local = []

    def load(src, dst):
        cp = pltpu.make_async_copy(src, dst, lsem.at[len(local)])
        cp.start()
        local.append(cp)
        return cp

    own = pl.ds(pl.multiple_of(tp * 1024, 1024), 1024)
    oth = pl.ds(pl.multiple_of(other * 1024, 1024), 1024)
    here, there = pl.ds(0, 1024), pl.ds(1024, 1024)

    def load2(a, b, rows, dst, to, w):
        return [load(a.at[rows], dst.at[to, pl.ds(0, w)]), load(b.at[rows], dst.at[to, pl.ds(w, w)])]

    c_tok = load(tok.at[0], tok_o)
    c_ld = [load(ld.at[h], ld_v.at[pl.ds(h, 1)]) for h in range(6)]
    c_gain = load(gain, gain_v)

    lane1 = iota((1, 128), 1)
    m0 = jnp.where(lane1 < 64, 1.0, 0.0).astype(bf16)
    m1 = jnp.where(lane1 < 64, 0.0, 1.0).astype(bf16)
    wmask[0:C] = jnp.where(iota((C, C), 0) > iota((C, C), 1), 1.0, 0.0).astype(bf16)
    wmask[C:] = jnp.where(iota((C, C), 0) > iota((C, C), 1), 0.0, 1.0).astype(bf16)
    biasc[...] = jnp.where(iota((C, C), 0) <= iota((C, C), 1), 0.0, NEG)

    for cp in c_ld:
        cp.wait()
    raw = ld_v[...]
    rows48 = jnp.concatenate([raw[:, c * C:(c + 1) * C] for c in range(NC)], axis=0)
    rows48 = jnp.where(lax.rem(iota((48, C), 0), 8) < 6, rows48, 0.0)
    upper = jnp.where(iota((C, C), 0) <= iota((C, C), 1), 1.0, 0.0).astype(bf16)
    parts = jnp.concatenate(split3(rows48), axis=0).astype(bf16)
    summed = dot(parts, upper)
    lc = summed[0:48] + summed[48:96] + summed[96:144]
    lcrow[...] = lc
    sr, sl = lax.rem(iota((24, 1152), 0), 8), iota((24, 1152), 1)
    head_of = jnp.where(sl < 384, lax.div(sl, 64), lax.div(sl - 384, 128))
    sel = jnp.where(sr == head_of, 1.0, 0.0).astype(bf16)
    exr[...] = jnp.exp(lc)
    before = jnp.zeros((1, 384), f32)
    before8 = jnp.zeros((8, 1), f32)
    for c in range(NC):
        p3 = jnp.concatenate(split3(lc[c * 8:(c + 1) * 8]), axis=0).astype(bf16)
        cols = t_dot(p3, sel)
        lch[pl.ds(c * C, C)] = cols[:, 384:]
        el[pl.ds(c * C, C)] = cols[:, :384]
        last = cols[C - 1:C, :384]
        tots[c:c + 1] = last
        before = before + last
        lc8 = lc[c * 8:(c + 1) * 8]
        frow[c * 8:(c + 1) * 8] = jnp.exp(lc8 + before8)
        before8 = before8 + lc8[:, C - 1:C]
    l_a[...] = jnp.zeros((8, 128), f32)
    for p in range(3):
        l_a[p:p + 1] = before[:, p * 128:(p + 1) * 128]

    c_gain.wait()
    c_tok.wait()
    c_kv = load2(wrk, wrv, own, wkv, here, 384)
    c_a = load2(wak, wav, own, wa, here, 128)
    c_kv2 = load2(wrk, wrv, oth, wkv, there, 384)
    c_a2 = load2(wak, wav, oth, wa, there, 128)
    c_q = load2(wrq, waq, own, wq, here, 384)
    c_q2 = load2(wrq, waq, oth, wq, there, 384)
    g_o = gain_v[:, own]
    g_p = gain_v[:, oth]

    def scale_rows(src, r0, g):
        x = src[pl.ds(r0, 64)].astype(f32)
        sq = x * x
        part = sq[:, 0:128]
        for j in range(1, 8):
            part = part + sq[:, j * 128:(j + 1) * 128]
        return (x * g).astype(bf16), part

    def own_rows(i, carry):
        r0 = pl.multiple_of(i * 64, 64)
        s, part = scale_rows(tok_o, r0, g_o)
        sc_o[pl.ds(r0, 64)] = s
        ssq[pl.ds(r0, 64)] = part
        return carry

    lax.fori_loop(0, T // 64, own_rows, 0)

    pl.semaphore_wait(barrier, len(greet))

    t_cp = []
    for r in range(2):
        rows = pl.ds(r * HALF, HALF)
        cp = pltpu.make_async_remote_copy(
            src_ref=tok_o.at[rows], dst_ref=tok_p.at[rows], send_sem=tsem.at[r], recv_sem=trec.at[r],
            device_id=peer, device_id_type=pl.DeviceIdType.MESH)
        cp.start()
        t_cp.append(cp)
    a_cp, al_cp, b_cp, bl_cp = [], [], [], []

    def send(src, dst, ss, rs, who, group):
        cp = pltpu.make_async_remote_copy(
            src_ref=src, dst_ref=dst, send_sem=ss, recv_sem=rs, device_id=who,
            device_id_type=pl.DeviceIdType.MESH)
        cp.start()
        group.append(cp)

    def arrived(src, dst, ss, rs, who):
        pltpu.make_async_remote_copy(
            src_ref=src, dst_ref=dst, send_sem=ss, recv_sem=rs, device_id=who,
            device_id_type=pl.DeviceIdType.MESH).wait_recv()

    for d in range(1, 4):
        send(l_a, buf_al.at[y], alsem.at[d - 1], alrec.at[y], at_y(d), al_cp)
    buf_al[y] = l_a[...]
    x_cp = []
    send(frow, frow_p, xsem.at[0], xrec.at[0], peer, x_cp)

    def first_half(acc, w):
        for r in range(2):
            rows = pl.ds(r * HALF, HALF)
            acc[rows] = dot(sc_o[rows], w[here])

    def wait_all(cps):
        for cp in cps:
            cp.wait()

    wait_all(c_kv)
    first_half(acc_kv, wkv)
    wait_all(c_a)
    first_half(acc_a, wa)

    c_small = [load(rgain, rgain_v), load(sink, sink_v)]
    c_wo = [load(wre, wo.at[0, pl.ds(0, 384)]), load(wao, wo.at[1, pl.ds(0, 384)])]

    wait_all(c_kv2)
    for r in range(2):
        t_cp[r].wait_recv()

        def peer_rows(i, carry):
            r0 = pl.multiple_of(r * HALF + i * 64, 64)
            s, part = scale_rows(tok_p, r0, g_p)
            tok_p[pl.ds(r0, 64)] = s
            total = jnp.sum(ssq[pl.ds(r0, 64)] + part, axis=1, keepdims=True)
            ssq[pl.ds(r0, 64)] = jnp.broadcast_to(lax.rsqrt(total / D + EPS), (64, 128))
            return carry

        lax.fori_loop(0, HALF // 64, peer_rows, 0)
        rows = pl.ds(r * HALF, HALF)
        res = acc_kv[rows] + dot(tok_p[rows], wkv[there])
        kv[rows] = (res * ssq[rows, 0:1]).astype(bf16)

    for d in range(1, 4):
        arrived(l_a, buf_al.at[y_at[d]], alsem.at[d - 1], alrec.at[y_at[d]], at_y(d))
    l_b[...] = buf_al[0] + buf_al[1] + buf_al[2] + buf_al[3]
    for d in range(1, 8):
        send(l_b, buf_bl.at[z], blsem.at[d - 1], blrec.at[z], at_z(d), bl_cp)
    buf_bl[z] = l_b[...]

    lo = iota((64, 128), 1) < 64
    s_p = [jnp.zeros((64, 128), f32) for _ in range(3)]
    for c in range(NC):
        rows = pl.ds(c * C, C)
        tot = tots[c:c + 1]
        for p in range(3):
            cols = pl.ds(p * 128, 128)
            tp_ = tot[:, p * 128:(p + 1) * 128]
            lcp = el[rows, cols]
            kd = (kv[rows, cols].astype(f32) * jnp.exp(tp_ - lcp)).astype(bf16)
            m = t_dot(kv[rows, pl.ds(384 + p * 128, 128)], kd)
            comp = jnp.where(lo, m[0:64], m[64:128])
            st[c, p] = s_p[p].astype(bf16)
            s_p[p] = jnp.exp(tp_) * s_p[p] + comp
    for p in range(3):
        for q in range(4):
            st_a[q, p] = s_p[p][q * 16:(q + 1) * 16].astype(bf16)

    for d in range(1, 4):
        send(st_a.at[y_at[d]], buf_a.at[y], asem.at[d - 1], arec.at[y], at_y(d), a_cp)
    buf_a[y] = st_a[y]

    w_cp = []
    for i, w in enumerate((wre, wao)):
        cp = pltpu.make_async_remote_copy(
            src_ref=w, dst_ref=wo.at[i, pl.ds(384, 384)], send_sem=wsem.at[i], recv_sem=wrec.at[i],
            device_id=peer, device_id_type=pl.DeviceIdType.MESH)
        cp.start()
        w_cp.append(cp)

    wait_all(c_a2)
    for r in range(2):
        rows = pl.ds(r * HALF, HALF)
        res = acc_a[rows] + dot(tok_p[rows], wa[there])
        akv[pl.ds(C + r * HALF, HALF)] = (res * ssq[rows, 0:1]).astype(bf16)
    halo = pltpu.make_async_remote_copy(
        src_ref=akv.at[pl.ds(T, C)], dst_ref=akv.at[pl.ds(0, C)], send_sem=hsem, recv_sem=hrec,
        device_id=nxt, device_id_type=pl.DeviceIdType.MESH)
    halo.start()
    wait_all(c_q + c_q2)
    for r in range(2):
        rows = pl.ds(r * HALF, HALF)
        res = dot(jnp.concatenate([sc_o[rows], tok_p[rows]], axis=1), wq[...])
        res = res * (ssq[rows, 0:1] * 0.125)
        qb[rows] = res[:, :384].astype(bf16)
        for p in range(3):
            two = res[:, 384 + p * 128:384 + (p + 1) * 128]
            swapped = pltpu.roll(two, 64, 1) if p != 1 else two
            for j in range(2):
                h = 2 * p + j
                val = ((swapped if h in (1, 4) else two).astype(bf16)) * (m0 if h < 3 else m1)
                for b in range(3):
                    qs[r * 3 + b, pl.ds(h * C, C)] = val[b * C:(b + 1) * C]

    def spread(s):
        return jnp.concatenate([s * m0, s * m1], axis=0)

    def ret_pair(i, carry):
        todo = []
        for u in range(2):
            c = lax.rem(other * 3 + 2 * i + u, NC)
            half, lanes = lax.div(c, 3), pl.ds(pl.multiple_of(lax.rem(c, 3) * C, C), C)
            rows = pl.ds(pl.multiple_of(c * C, C), C)
            eight = pl.ds(pl.multiple_of(c * 8, 8), 8)
            for p in range(3):
                q2 = qb[rows, pl.ds(p * 128, 128)]
                s = dot_t(kv[rows, pl.ds(p * 128, 128)], jnp.concatenate([q2 * m0, q2 * m1], axis=0))
                todo.append((p, half, lanes, rows, lcrow[eight], exr[eight], s, dot_t(spread(st[c, p]), q2)))
        for p, half, lanes, rows, lrows, erows, s, past in todo:
            ws = []
            for j in range(2):
                h = 2 * p + j
                gap = lrows[h:h + 1] - lch[rows, pl.ds(h * 128, 128)] + biasc[...]
                ws.append((s[:, j * C:(j + 1) * C] * jnp.exp(gap)).astype(bf16))
            o = t_dot(kv[rows, pl.ds(384 + p * 128, 128)], jnp.concatenate(ws, axis=1))
            for j in range(2):
                h, r = 2 * p + j, slice(j * 64, (j + 1) * 64)
                inner[half, pl.ds(h * 64, 64), lanes] = o[r, j * C:(j + 1) * C] + past[r] * erows[h:h + 1]
        return carry

    mine = pl.ds(pl.multiple_of(tp * HALF, HALF), HALF)
    theirs = pl.ds(pl.multiple_of(other * HALF, HALF), HALF)

    for d in range(1, 4):
        arrived(st_a.at[0], buf_a.at[y_at[d]], asem.at[d - 1], arec.at[y_at[d]], at_y(d))
    for p in range(3):
        e = jnp.zeros((16, 128), f32)
        for yy in range(4):
            lyy = buf_al[yy][p:p + 1]
            e = jnp.exp(lyy) * e + buf_a[yy, p].astype(f32)
        g_b[p] = e.astype(bf16)
    for d in range(1, 8):
        send(g_b, buf_b.at[z], bsem.at[d - 1], brec.at[z], at_z(d), b_cp)
    buf_b[z] = g_b[...]

    send(qb.at[theirs], q_p, xsem.at[1], xrec.at[1], peer, x_cp)
    lax.fori_loop(0, 2, ret_pair, 0)

    wait_all(c_small)
    halo.wait_recv()
    for p in range(3):
        g = jnp.broadcast_to(rgain_v[pl.ds(p * C, C)].reshape(1, C), (C, C))
        gcol[pl.ds(p * C, C)] = jnp.transpose(g)
    sink_row = jnp.concatenate(
        [jnp.broadcast_to(sink_v[0:1, h:h + 1], (1, C)) for h in range(6)], axis=1)

    def att_half(half):
        is_own = iota((C, C), 0) <= iota((C, C), 1)

        def scores(i):
            n = half * 3 + i
            return dot_t(akv[pl.ds(pl.multiple_of(n * C, C), 2 * C), pl.ds(0, 128)], qs[n])

        def block(i, s):
            n = half * 3 + i
            ws, scale = [], []
            for h in range(6):
                hc = slice(h * C, (h + 1) * C)
                past = s[:C, hc]
                if i == 0:
                    past = jnp.where((n == 0) & (sp == 0), NEG, past)
                v = jnp.where(is_own, s[C:, hc], past)
                sk = sink_row[:, hc]
                top = jnp.maximum(jnp.max(v, axis=0, keepdims=True), sk)
                e = jnp.exp(v - top)
                scale.append(1.0 / (jnp.sum(e, axis=0, keepdims=True) + jnp.exp(sk - top)))
                eb = e.astype(bf16)
                ws.append(jnp.concatenate([eb * wmask[0:C], eb * wmask[C:]], axis=0))
            bandr = pl.ds(pl.multiple_of(n * C, C), 2 * C)
            return scale, t_dot(akv[bandr, pl.ds(128, 128)], jnp.concatenate(ws, axis=1))

        ahead = scores(0)
        for i in range(3):
            s = ahead
            if i < 2:
                ahead = scores(i + 1)
            scale, o = block(i, s)
            for h in range(6):
                r0 = 64 if h >= 3 else 0
                att[half, pl.ds(h * 64, 64), pl.ds(i * C, C)] = (
                    o[r0:r0 + 64, h * C:(h + 1) * C] * scale[h]).astype(bf16)

    o_cp = []
    att_half(other)
    send(inner.at[other], in_p, xsem.at[2], xrec.at[2], peer, x_cp)
    send(gcol, gcol_p, xsem.at[3], xrec.at[3], peer, x_cp)
    send(att.at[other], att_p, osem.at[0], orec.at[0], peer, o_cp)
    att_half(tp)

    for d in range(1, 8):
        arrived(g_b, buf_b.at[z_at[d]], bsem.at[d - 1], brec.at[z_at[d]], at_z(d))
        arrived(l_b, buf_bl.at[z_at[d]], blsem.at[d - 1], blrec.at[z_at[d]], at_z(d))
    for p in range(3):
        e = jnp.zeros((16, 128), f32)
        for zz in range(7):
            step = jnp.exp(buf_bl[zz][p:p + 1]) * e + buf_b[zz, p].astype(f32)
            e = jnp.where(zz < z, step, e)
        for yy in range(4):
            s_c[yy, p] = e.astype(bf16)
            e = jnp.exp(buf_al[yy][p:p + 1]) * e + buf_a[yy, p].astype(f32)
    c_cp = []
    for d in range(1, 4):
        send(s_c.at[y_at[d]], buf_c.at[0, y], csem.at[d - 1], crec.at[0, y], at_y(d), c_cp)
        send(s_c.at[y_at[d]], buf_c.at[1, y], csem.at[d + 2], crec.at[1, y], across_y(d), c_cp)
    send(s_c.at[y], buf_c.at[1, y], csem.at[6], crec.at[1, y], peer, c_cp)
    buf_c[0, y] = s_c[y]

    ret_pair(2, 0)

    wait_all(c_wo)
    w_cp[0].wait_recv()
    w_cp[1].wait_recv()
    o_cp[0].wait_recv()
    lhs = jnp.concatenate([att[tp], att_p[...]], axis=0)
    for j in range(4):
        cols = pl.ds(j * 512, 512)
        oacc[:, cols] = t_dot(lhs, wo[1, :, cols])

    for cp in x_cp:
        cp.wait_recv()
    for d in range(1, 4):
        arrived(s_c.at[0], buf_c.at[0, y_at[d]], csem.at[0], crec.at[0, y_at[d]], at_y(d))
    for d in range(4):
        arrived(s_c.at[0], buf_c.at[1, y_at[d]], csem.at[0], crec.at[1, y_at[d]], peer)
    sides = ((inner.at[tp], qb.at[mine], frow, gcol), (in_p, q_p, frow_p, gcol_p))
    for side, (inn, qrows, factors, gains) in enumerate(sides):
        for p in range(3):
            big = spread(jnp.concatenate([buf_c[side, q, p] for q in range(4)], axis=0))
            car = dot_t(big, qrows[:, p * 128:(p + 1) * 128])
            for b in range(3):
                lanes = slice(b * C, (b + 1) * C)
                f8 = factors[pl.ds(pl.multiple_of((tp * 3 + b) * 8, 8), 8)]
                for j in range(2):
                    h = 2 * p + j
                    hr = slice(h * 64, (h + 1) * 64)
                    full = inn[hr, lanes] + car[j * 64:(j + 1) * 64, lanes] * f8[h:h + 1]
                    ms = jnp.sum(full * full, axis=0, keepdims=True) * (1.0 / 64)
                    ret[side * 384 + h * 64:side * 384 + (h + 1) * 64, lanes] = (
                        full * lax.rsqrt(ms + EPS) * gains[hr]).astype(bf16)
    for j in range(2):
        cols = pl.ds(j * 1024, 1024)
        out[0, :, cols] = (oacc[:, cols] + t_dot(ret[...], wo[0, :, cols])).astype(bf16)

    for cp in t_cp + w_cp + a_cp + al_cp + b_cp + bl_cp + c_cp + o_cp + x_cp + [halo]:
        cp.wait_send()


def shards(tokens, in_gain, ret_query, ret_key, ret_value, att_query, att_key, att_value,
           log_decay, ret_gain, sink_logit, retentive_exit_matrix, out_att):
    hbm = pl.BlockSpec(memory_space=pltpu.HBM)
    V = pltpu.VMEM
    DMA = pltpu.SemaphoreType.DMA
    scratch = [
        V((1, D), f32), V((384,), f32), V((1, 6), f32), V((8, T), f32),
        V((T, 1024), bf16), V((T, 1024), bf16), V((T, 1024), bf16), V((T, 128), f32),
        V((D, 768), bf16), V((D, 768), bf16), V((D, 256), bf16),
        V((T, 768), f32), V((T, 256), f32),
        V((T, 768), bf16), V((T, 384), bf16), V((T + C, 256), bf16), V((NC, 768, 128), bf16),
        V((48, 128), f32), V((48, 128), f32), V((48, 128), f32), V((T, 768), f32), V((T, 384), f32), V((8, 384), f32),
        V((NC, 3, 64, 128), bf16), V((2, 384, HALF), f32), V((384, 128), f32),
        V((2 * C, C), bf16), V((C, C), f32),
        V((4, 3, 16, 128), bf16), V((4, 3, 16, 128), bf16), V((8, 128), f32), V((4, 8, 128), f32),
        V((3, 16, 128), bf16), V((8, 3, 16, 128), bf16), V((8, 128), f32), V((8, 8, 128), f32),
        V((4, 3, 16, 128), bf16), V((2, 4, 3, 16, 128), bf16),
        V((2, 768, D), bf16), V((2, 384, HALF), bf16), V((384, HALF), bf16), V((768, HALF), bf16),
        V((HALF, D), f32), V((384, HALF), f32), V((HALF, 384), bf16), V((48, 128), f32), V((384, 128), f32),
        DMA((24,)), DMA((2,)), DMA((2,)), DMA((2,)), DMA((2,)), DMA(()), DMA(()),
        DMA((3,)), DMA((4,)), DMA((3,)), DMA((4,)), DMA((7,)), DMA((8,)), DMA((7,)), DMA((8,)),
        DMA((7,)), DMA((2, 4)), DMA((1,)), DMA((1,)), DMA((4,)), DMA((4,)),
    ]
    return pl.pallas_call(
        kernel,
        out_shape=jax.ShapeDtypeStruct((1, HALF, D), bf16),
        in_specs=[hbm] * 13,
        out_specs=pl.BlockSpec(memory_space=pltpu.VMEM),
        scratch_shapes=scratch,
        compiler_params=pltpu.CompilerParams(
            collective_id=0, has_side_effects=True, vmem_limit_bytes=48 * 1024 * 1024),
    )(*(pltpu.with_memory_space_constraint(arg, pltpu.HBM) for arg in (
        tokens, in_gain.reshape(1, D), ret_query, ret_key, ret_value, att_query, att_key, att_value,
        jnp.transpose(log_decay, (1, 0, 2)), ret_gain, sink_logit.reshape(1, 6), retentive_exit_matrix, out_att,
    )))


def solution(mesh):
    placed = (
        P("fs", "sp", "tp"), P(), P(None, "tp"), P(None, "tp"), P(None, "tp"), P(None, "tp"),
        P(None, "tp"), P(None, "tp"), P("fs", "tp", "sp"), P("tp"), P("tp"), P("tp", None), P("tp", None),
    )
    return jax.shard_map(
        shards, mesh=mesh, in_specs=placed, out_specs=P("fs", ("sp", "tp"), None), check_vma=False)
```

```python
import functools

import jax
import jax.numpy as jnp
from jax import lax
from jax.experimental import pallas as pl
from jax.experimental.pallas import tpu as pltpu
from jax.sharding import PartitionSpec as P

EPS = 1e-06
D = 2048
T = 768
HALF = 384
C = 128
NC = 6
YS = (2, 1, 3)
ZS = (4, 3, 5, 2, 6, 1, 7)
NEG = float("-inf")
f32 = jnp.float32
bf16 = jnp.bfloat16


def dot(a, b):
    return jnp.dot(a, b, preferred_element_type=f32)


def dot_t(a, b):
    return lax.dot_general(a, b, (((1,), (1,)), ((), ())), preferred_element_type=f32)


def t_dot(a, b):
    return lax.dot_general(a, b, (((0,), (0,)), ((), ())), preferred_element_type=f32)


def split3(x):
    a = x.astype(bf16).astype(f32)
    r = x - a
    b = r.astype(bf16).astype(f32)
    return a, b, (r - b).astype(bf16).astype(f32)


def iota(shape, dim):
    return lax.broadcasted_iota(jnp.int32, shape, dim)


def kernel(
    tok, gain, wrq, wrk, wrv, waq, wak, wav, ld, rgain, sink, wre, wao,
    out,
    gain_v, rgain_v, sink_v, ld_v,
    tok_o, tok_p, sc_o, ssq,
    wkv, wq, wa, acc_kv, acc_a,
    kv, qb, akv, qs,
    lcrow, exr, frow, lch, el, tots, st, inner, gcol,
    wmask, biasc,
    st_a, buf_a, l_a, buf_al, g_b, buf_b, l_b, buf_bl, s_c, buf_c,
    wo, att, att_p, ret, oacc, in_p, q_p, frow_p, gcol_p,
    lsem, tsem, trec, wsem, wrec, hsem, hrec,
    asem, arec, alsem, alrec, bsem, brec, blsem, blrec, csem, crec, osem, orec, xsem, xrec,
):
    sp = lax.axis_index("sp")
    tp = lax.axis_index("tp")
    y = lax.rem(sp, 4)
    z = lax.div(sp, 4)
    other = 1 - tp
    peer = {"tp": other}
    y_at = [lax.rem(y + d, 4) for d in range(4)]
    z_at = [lax.rem(z + d, 8) for d in range(8)]

    def at_y(d):
        return {"sp": z * 4 + y_at[d]}

    def at_z(d):
        return {"sp": z_at[d] * 4 + y}

    def across_y(d):
        return {"sp": z * 4 + y_at[d], "tp": other}

    nxt = {"sp": lax.rem(sp + 1, 32)}
    prv = {"sp": lax.rem(sp + 31, 32)}

    barrier = pltpu.get_barrier_semaphore()
    greet = [at_z(d) for d in ZS] + [at_y(d) for d in YS] + [across_y(d) for d in YS] + [prv, peer]
    for who in greet:
        pl.semaphore_signal(barrier, inc=1, device_id=who, device_id_type=pl.DeviceIdType.MESH)

    local = []

    def load(src, dst):
        cp = pltpu.make_async_copy(src, dst, lsem.at[len(local)])
        cp.start()
        local.append(cp)
        return cp

    own = pl.ds(pl.multiple_of(tp * 1024, 1024), 1024)
    oth = pl.ds(pl.multiple_of(other * 1024, 1024), 1024)
    here, there = pl.ds(0, 1024), pl.ds(1024, 1024)

    def load2(a, b, rows, dst, to, w):
        return [load(a.at[rows], dst.at[to, pl.ds(0, w)]), load(b.at[rows], dst.at[to, pl.ds(w, w)])]

    c_tok = load(tok.at[0], tok_o)
    c_ld = [load(ld.at[h], ld_v.at[pl.ds(h, 1)]) for h in range(6)]
    c_gain = load(gain, gain_v)

    lane1 = iota((1, 128), 1)
    m0 = jnp.where(lane1 < 64, 1.0, 0.0).astype(bf16)
    m1 = jnp.where(lane1 < 64, 0.0, 1.0).astype(bf16)
    wmask[0:C] = jnp.where(iota((C, C), 0) > iota((C, C), 1), 1.0, 0.0).astype(bf16)
    wmask[C:] = jnp.where(iota((C, C), 0) > iota((C, C), 1), 0.0, 1.0).astype(bf16)
    biasc[...] = jnp.where(iota((C, C), 0) <= iota((C, C), 1), 0.0, NEG)

    for cp in c_ld:
        cp.wait()
    raw = ld_v[...]
    rows48 = jnp.concatenate([raw[:, c * C:(c + 1) * C] for c in range(NC)], axis=0)
    rows48 = jnp.where(lax.rem(iota((48, C), 0), 8) < 6, rows48, 0.0)
    upper = jnp.where(iota((C, C), 0) <= iota((C, C), 1), 1.0, 0.0).astype(bf16)
    parts = jnp.concatenate(split3(rows48), axis=0).astype(bf16)
    summed = dot(parts, upper)
    lc = summed[0:48] + summed[48:96] + summed[96:144]
    lcrow[...] = lc
    sr, sl = lax.rem(iota((24, 1152), 0), 8), iota((24, 1152), 1)
    head_of = jnp.where(sl < 384, lax.div(sl, 64), lax.div(sl - 384, 128))
    sel = jnp.where(sr == head_of, 1.0, 0.0).astype(bf16)
    exr[...] = jnp.exp(lc)
    before = jnp.zeros((1, 384), f32)
    before8 = jnp.zeros((8, 1), f32)
    for c in range(NC):
        p3 = jnp.concatenate(split3(lc[c * 8:(c + 1) * 8]), axis=0).astype(bf16)
        cols = t_dot(p3, sel)
        lch[pl.ds(c * C, C)] = cols[:, 384:]
        el[pl.ds(c * C, C)] = cols[:, :384]
        last = cols[C - 1:C, :384]
        tots[c:c + 1] = last
        before = before + last
        lc8 = lc[c * 8:(c + 1) * 8]
        frow[c * 8:(c + 1) * 8] = jnp.exp(lc8 + before8)
        before8 = before8 + lc8[:, C - 1:C]
    l_a[...] = jnp.zeros((8, 128), f32)
    for p in range(3):
        l_a[p:p + 1] = before[:, p * 128:(p + 1) * 128]

    c_gain.wait()
    c_tok.wait()
    c_kv = load2(wrk, wrv, own, wkv, here, 384)
    c_a = load2(wak, wav, own, wa, here, 128)
    c_kv2 = load2(wrk, wrv, oth, wkv, there, 384)
    c_a2 = load2(wak, wav, oth, wa, there, 128)
    c_q = load2(wrq, waq, own, wq, here, 384)
    c_q2 = load2(wrq, waq, oth, wq, there, 384)
    g_o = gain_v[:, own]
    g_p = gain_v[:, oth]

    def scale_rows(src, r0, g):
        x = src[pl.ds(r0, 64)].astype(f32)
        sq = x * x
        part = sq[:, 0:128]
        for j in range(1, 8):
            part = part + sq[:, j * 128:(j + 1) * 128]
        return (x * g).astype(bf16), part

    def own_rows(i, carry):
        r0 = pl.multiple_of(i * 64, 64)
        s, part = scale_rows(tok_o, r0, g_o)
        sc_o[pl.ds(r0, 64)] = s
        ssq[pl.ds(r0, 64)] = part
        return carry

    lax.fori_loop(0, T // 64, own_rows, 0)

    pl.semaphore_wait(barrier, len(greet))

    t_cp = []
    for r in range(2):
        rows = pl.ds(r * HALF, HALF)
        cp = pltpu.make_async_remote_copy(
            src_ref=tok_o.at[rows], dst_ref=tok_p.at[rows], send_sem=tsem.at[r], recv_sem=trec.at[r],
            device_id=peer, device_id_type=pl.DeviceIdType.MESH)
        cp.start()
        t_cp.append(cp)
    a_cp, al_cp, b_cp, bl_cp = [], [], [], []

    def send(src, dst, ss, rs, who, group):
        cp = pltpu.make_async_remote_copy(
            src_ref=src, dst_ref=dst, send_sem=ss, recv_sem=rs, device_id=who,
            device_id_type=pl.DeviceIdType.MESH)
        cp.start()
        group.append(cp)

    def arrived(src, dst, ss, rs, who):
        pltpu.make_async_remote_copy(
            src_ref=src, dst_ref=dst, send_sem=ss, recv_sem=rs, device_id=who,
            device_id_type=pl.DeviceIdType.MESH).wait_recv()

    for d in YS:
        send(l_a, buf_al.at[y], alsem.at[d - 1], alrec.at[y], at_y(d), al_cp)
    buf_al[y] = l_a[...]
    x_cp = []
    send(frow, frow_p, xsem.at[0], xrec.at[0], peer, x_cp)

    def first_half(acc, w):
        for r in range(2):
            rows = pl.ds(r * HALF, HALF)
            acc[rows] = dot(sc_o[rows], w[here])

    def wait_all(cps):
        for cp in cps:
            cp.wait()

    wait_all(c_kv)
    first_half(acc_kv, wkv)
    wait_all(c_a)
    first_half(acc_a, wa)

    c_small = [load(rgain, rgain_v), load(sink, sink_v)]
    c_wo = [load(wre, wo.at[0, pl.ds(0, 384)]), load(wao, wo.at[1, pl.ds(0, 384)])]

    wait_all(c_kv2)
    for r in range(2):
        t_cp[r].wait_recv()

        def peer_rows(i, carry):
            r0 = pl.multiple_of(r * HALF + i * 64, 64)
            s, part = scale_rows(tok_p, r0, g_p)
            tok_p[pl.ds(r0, 64)] = s
            total = jnp.sum(ssq[pl.ds(r0, 64)] + part, axis=1, keepdims=True)
            ssq[pl.ds(r0, 64)] = jnp.broadcast_to(lax.rsqrt(total / D + EPS), (64, 128))
            return carry

        lax.fori_loop(0, HALF // 64, peer_rows, 0)
        rows = pl.ds(r * HALF, HALF)
        res = acc_kv[rows] + dot(tok_p[rows], wkv[there])
        kv[rows] = (res * ssq[rows, 0:1]).astype(bf16)

    for d in range(1, 4):
        arrived(l_a, buf_al.at[y_at[d]], alsem.at[d - 1], alrec.at[y_at[d]], at_y(d))
    l_b[...] = buf_al[0] + buf_al[1] + buf_al[2] + buf_al[3]
    for d in ZS:
        send(l_b, buf_bl.at[z], blsem.at[d - 1], blrec.at[z], at_z(d), bl_cp)
    buf_bl[z] = l_b[...]

    lo = iota((64, 128), 1) < 64
    s_p = [jnp.zeros((64, 128), f32) for _ in range(3)]
    for c in range(NC):
        rows = pl.ds(c * C, C)
        tot = tots[c:c + 1]
        for p in range(3):
            cols = pl.ds(p * 128, 128)
            tp_ = tot[:, p * 128:(p + 1) * 128]
            lcp = el[rows, cols]
            kd = (kv[rows, cols].astype(f32) * jnp.exp(tp_ - lcp)).astype(bf16)
            m = t_dot(kv[rows, pl.ds(384 + p * 128, 128)], kd)
            comp = jnp.where(lo, m[0:64], m[64:128])
            st[c, p] = s_p[p].astype(bf16)
            s_p[p] = jnp.exp(tp_) * s_p[p] + comp
    for p in range(3):
        for q in range(4):
            st_a[q, p] = s_p[p][q * 16:(q + 1) * 16].astype(bf16)

    for d in YS:
        send(st_a.at[y_at[d]], buf_a.at[y], asem.at[d - 1], arec.at[y], at_y(d), a_cp)
    buf_a[y] = st_a[y]

    w_cp = []
    for i, w in enumerate((wre, wao)):
        cp = pltpu.make_async_remote_copy(
            src_ref=w, dst_ref=wo.at[i, pl.ds(384, 384)], send_sem=wsem.at[i], recv_sem=wrec.at[i],
            device_id=peer, device_id_type=pl.DeviceIdType.MESH)
        cp.start()
        w_cp.append(cp)

    wait_all(c_a2)
    for r in range(2):
        rows = pl.ds(r * HALF, HALF)
        res = acc_a[rows] + dot(tok_p[rows], wa[there])
        akv[pl.ds(C + r * HALF, HALF)] = (res * ssq[rows, 0:1]).astype(bf16)
    halo = pltpu.make_async_remote_copy(
        src_ref=akv.at[pl.ds(T, C)], dst_ref=akv.at[pl.ds(0, C)], send_sem=hsem, recv_sem=hrec,
        device_id=nxt, device_id_type=pl.DeviceIdType.MESH)
    halo.start()
    wait_all(c_q + c_q2)
    for r in range(2):
        rows = pl.ds(r * HALF, HALF)
        res = dot(jnp.concatenate([sc_o[rows], tok_p[rows]], axis=1), wq[...])
        res = res * (ssq[rows, 0:1] * 0.125)
        qb[rows] = res[:, :384].astype(bf16)
        for p in range(3):
            two = res[:, 384 + p * 128:384 + (p + 1) * 128]
            swapped = pltpu.roll(two, 64, 1) if p != 1 else two
            for j in range(2):
                h = 2 * p + j
                val = ((swapped if h in (1, 4) else two).astype(bf16)) * (m0 if h < 3 else m1)
                for b in range(3):
                    qs[r * 3 + b, pl.ds(h * C, C)] = val[b * C:(b + 1) * C]

    def spread(s):
        return jnp.concatenate([s * m0, s * m1], axis=0)

    def ret_pair(i, carry):
        todo = []
        for u in range(2):
            c = lax.rem(other * 3 + 2 * i + u, NC)
            half, lanes = lax.div(c, 3), pl.ds(pl.multiple_of(lax.rem(c, 3) * C, C), C)
            rows = pl.ds(pl.multiple_of(c * C, C), C)
            eight = pl.ds(pl.multiple_of(c * 8, 8), 8)
            for p in range(3):
                q2 = qb[rows, pl.ds(p * 128, 128)]
                s = dot_t(kv[rows, pl.ds(p * 128, 128)], jnp.concatenate([q2 * m0, q2 * m1], axis=0))
                todo.append((p, half, lanes, rows, lcrow[eight], exr[eight], s, dot_t(spread(st[c, p]), q2)))
        for p, half, lanes, rows, lrows, erows, s, past in todo:
            ws = []
            for j in range(2):
                h = 2 * p + j
                gap = lrows[h:h + 1] - lch[rows, pl.ds(h * 128, 128)] + biasc[...]
                ws.append((s[:, j * C:(j + 1) * C] * jnp.exp(gap)).astype(bf16))
            o = t_dot(kv[rows, pl.ds(384 + p * 128, 128)], jnp.concatenate(ws, axis=1))
            for j in range(2):
                h, r = 2 * p + j, slice(j * 64, (j + 1) * 64)
                inner[half, pl.ds(h * 64, 64), lanes] = o[r, j * C:(j + 1) * C] + past[r] * erows[h:h + 1]
        return carry

    mine = pl.ds(pl.multiple_of(tp * HALF, HALF), HALF)
    theirs = pl.ds(pl.multiple_of(other * HALF, HALF), HALF)

    for d in range(1, 4):
        arrived(st_a.at[0], buf_a.at[y_at[d]], asem.at[d - 1], arec.at[y_at[d]], at_y(d))
    for p in range(3):
        e = jnp.zeros((16, 128), f32)
        for yy in range(4):
            lyy = buf_al[yy][p:p + 1]
            e = jnp.exp(lyy) * e + buf_a[yy, p].astype(f32)
        g_b[p] = e.astype(bf16)
    for d in ZS:
        send(g_b, buf_b.at[z], bsem.at[d - 1], brec.at[z], at_z(d), b_cp)
    buf_b[z] = g_b[...]

    send(qb.at[theirs], q_p, xsem.at[1], xrec.at[1], peer, x_cp)
    lax.fori_loop(0, 2, ret_pair, 0)

    wait_all(c_small)
    halo.wait_recv()
    for p in range(3):
        g = jnp.broadcast_to(rgain_v[pl.ds(p * C, C)].reshape(1, C), (C, C))
        gcol[pl.ds(p * C, C)] = jnp.transpose(g)
    sink_row = jnp.concatenate(
        [jnp.broadcast_to(sink_v[0:1, h:h + 1], (1, C)) for h in range(6)], axis=1)

    def att_half(half):
        is_own = iota((C, C), 0) <= iota((C, C), 1)

        def scores(i):
            n = half * 3 + i
            return dot_t(akv[pl.ds(pl.multiple_of(n * C, C), 2 * C), pl.ds(0, 128)], qs[n])

        def block(i, s):
            n = half * 3 + i
            ws, scale = [], []
            for h in range(6):
                hc = slice(h * C, (h + 1) * C)
                past = s[:C, hc]
                if i == 0:
                    past = jnp.where((n == 0) & (sp == 0), NEG, past)
                v = jnp.where(is_own, s[C:, hc], past)
                sk = sink_row[:, hc]
                top = jnp.maximum(jnp.max(v, axis=0, keepdims=True), sk)
                e = jnp.exp(v - top)
                scale.append(1.0 / (jnp.sum(e, axis=0, keepdims=True) + jnp.exp(sk - top)))
                eb = e.astype(bf16)
                ws.append(jnp.concatenate([eb * wmask[0:C], eb * wmask[C:]], axis=0))
            bandr = pl.ds(pl.multiple_of(n * C, C), 2 * C)
            return scale, t_dot(akv[bandr, pl.ds(128, 128)], jnp.concatenate(ws, axis=1))

        ahead = scores(0)
        for i in range(3):
            s = ahead
            if i < 2:
                ahead = scores(i + 1)
            scale, o = block(i, s)
            for h in range(6):
                r0 = 64 if h >= 3 else 0
                att[half, pl.ds(h * 64, 64), pl.ds(i * C, C)] = (
                    o[r0:r0 + 64, h * C:(h + 1) * C] * scale[h]).astype(bf16)

    o_cp = []
    att_half(other)
    send(inner.at[other], in_p, xsem.at[2], xrec.at[2], peer, x_cp)
    send(gcol, gcol_p, xsem.at[3], xrec.at[3], peer, x_cp)
    send(att.at[other], att_p, osem.at[0], orec.at[0], peer, o_cp)
    att_half(tp)

    for d in range(1, 8):
        arrived(g_b, buf_b.at[z_at[d]], bsem.at[d - 1], brec.at[z_at[d]], at_z(d))
        arrived(l_b, buf_bl.at[z_at[d]], blsem.at[d - 1], blrec.at[z_at[d]], at_z(d))
    for p in range(3):
        e = jnp.zeros((16, 128), f32)
        for zz in range(7):
            step = jnp.exp(buf_bl[zz][p:p + 1]) * e + buf_b[zz, p].astype(f32)
            e = jnp.where(zz < z, step, e)
        for yy in range(4):
            s_c[yy, p] = e.astype(bf16)
            e = jnp.exp(buf_al[yy][p:p + 1]) * e + buf_a[yy, p].astype(f32)
    c_cp = []
    for d in YS:
        send(s_c.at[y_at[d]], buf_c.at[0, y], csem.at[d - 1], crec.at[0, y], at_y(d), c_cp)
        send(s_c.at[y_at[d]], buf_c.at[1, y], csem.at[d + 2], crec.at[1, y], across_y(d), c_cp)
    send(s_c.at[y], buf_c.at[1, y], csem.at[6], crec.at[1, y], peer, c_cp)
    buf_c[0, y] = s_c[y]

    ret_pair(2, 0)

    wait_all(c_wo)
    w_cp[0].wait_recv()
    w_cp[1].wait_recv()
    o_cp[0].wait_recv()
    lhs = jnp.concatenate([att[tp], att_p[...]], axis=0)
    for j in range(4):
        cols = pl.ds(j * 512, 512)
        oacc[:, cols] = t_dot(lhs, wo[1, :, cols])

    for cp in x_cp:
        cp.wait_recv()
    for d in range(1, 4):
        arrived(s_c.at[0], buf_c.at[0, y_at[d]], csem.at[0], crec.at[0, y_at[d]], at_y(d))
    for d in range(4):
        arrived(s_c.at[0], buf_c.at[1, y_at[d]], csem.at[0], crec.at[1, y_at[d]], peer)
    sides = ((inner.at[tp], qb.at[mine], frow, gcol), (in_p, q_p, frow_p, gcol_p))
    for side, (inn, qrows, factors, gains) in enumerate(sides):
        for p in range(3):
            big = spread(jnp.concatenate([buf_c[side, q, p] for q in range(4)], axis=0))
            car = dot_t(big, qrows[:, p * 128:(p + 1) * 128])
            for b in range(3):
                lanes = slice(b * C, (b + 1) * C)
                f8 = factors[pl.ds(pl.multiple_of((tp * 3 + b) * 8, 8), 8)]
                for j in range(2):
                    h = 2 * p + j
                    hr = slice(h * 64, (h + 1) * 64)
                    full = inn[hr, lanes] + car[j * 64:(j + 1) * 64, lanes] * f8[h:h + 1]
                    ms = jnp.sum(full * full, axis=0, keepdims=True) * (1.0 / 64)
                    ret[side * 384 + h * 64:side * 384 + (h + 1) * 64, lanes] = (
                        full * lax.rsqrt(ms + EPS) * gains[hr]).astype(bf16)
    for j in range(2):
        cols = pl.ds(j * 1024, 1024)
        out[0, :, cols] = (oacc[:, cols] + t_dot(ret[...], wo[0, :, cols])).astype(bf16)

    for cp in t_cp + w_cp + a_cp + al_cp + b_cp + bl_cp + c_cp + o_cp + x_cp + [halo]:
        cp.wait_send()


def shards(tokens, in_gain, ret_query, ret_key, ret_value, att_query, att_key, att_value,
           log_decay, ret_gain, sink_logit, retentive_exit_matrix, out_att):
    hbm = pl.BlockSpec(memory_space=pltpu.HBM)
    V = pltpu.VMEM
    DMA = pltpu.SemaphoreType.DMA
    scratch = [
        V((1, D), f32), V((384,), f32), V((1, 6), f32), V((8, T), f32),
        V((T, 1024), bf16), V((T, 1024), bf16), V((T, 1024), bf16), V((T, 128), f32),
        V((D, 768), bf16), V((D, 768), bf16), V((D, 256), bf16),
        V((T, 768), f32), V((T, 256), f32),
        V((T, 768), bf16), V((T, 384), bf16), V((T + C, 256), bf16), V((NC, 768, 128), bf16),
        V((48, 128), f32), V((48, 128), f32), V((48, 128), f32), V((T, 768), f32), V((T, 384), f32), V((8, 384), f32),
        V((NC, 3, 64, 128), bf16), V((2, 384, HALF), f32), V((384, 128), f32),
        V((2 * C, C), bf16), V((C, C), f32),
        V((4, 3, 16, 128), bf16), V((4, 3, 16, 128), bf16), V((8, 128), f32), V((4, 8, 128), f32),
        V((3, 16, 128), bf16), V((8, 3, 16, 128), bf16), V((8, 128), f32), V((8, 8, 128), f32),
        V((4, 3, 16, 128), bf16), V((2, 4, 3, 16, 128), bf16),
        V((2, 768, D), bf16), V((2, 384, HALF), bf16), V((384, HALF), bf16), V((768, HALF), bf16),
        V((HALF, D), f32), V((384, HALF), f32), V((HALF, 384), bf16), V((48, 128), f32), V((384, 128), f32),
        DMA((24,)), DMA((2,)), DMA((2,)), DMA((2,)), DMA((2,)), DMA(()), DMA(()),
        DMA((3,)), DMA((4,)), DMA((3,)), DMA((4,)), DMA((7,)), DMA((8,)), DMA((7,)), DMA((8,)),
        DMA((7,)), DMA((2, 4)), DMA((1,)), DMA((1,)), DMA((4,)), DMA((4,)),
    ]
    return pl.pallas_call(
        kernel,
        out_shape=jax.ShapeDtypeStruct((1, HALF, D), bf16),
        in_specs=[hbm] * 13,
        out_specs=pl.BlockSpec(memory_space=pltpu.VMEM),
        scratch_shapes=scratch,
        compiler_params=pltpu.CompilerParams(
            collective_id=0, has_side_effects=True, vmem_limit_bytes=48 * 1024 * 1024),
    )(*(pltpu.with_memory_space_constraint(arg, pltpu.HBM) for arg in (
        tokens, in_gain.reshape(1, D), ret_query, ret_key, ret_value, att_query, att_key, att_value,
        jnp.transpose(log_decay, (1, 0, 2)), ret_gain, sink_logit.reshape(1, 6), retentive_exit_matrix, out_att,
    )))


def solution(mesh):
    placed = (
        P("fs", "sp", "tp"), P(), P(None, "tp"), P(None, "tp"), P(None, "tp"), P(None, "tp"),
        P(None, "tp"), P(None, "tp"), P("fs", "tp", "sp"), P("tp"), P("tp"), P("tp", None), P("tp", None),
    )
    return jax.shard_map(
        shards, mesh=mesh, in_specs=placed, out_specs=P("fs", ("sp", "tp"), None), check_vma=False)
```
